32 devices in a mesh: grp: 2 (over y), sp: 4 (over z), tp: 4 (over x, core).
Axes of the slice: x: 2, y: 2, z: 4, core: 2. Of those that a mesh axis runs over, the one named last changes fastest.
Arguments:
- tokens: bfloat16 [256, 8, 2048], P(('sp', 'tp'), 'grp'), parts along dimension 1, may hold values from -6 to 6
- norm_gain: float32 [2048], replicated, may hold values from 0.1 to 1.9
- w_query: bfloat16 [2048, 2048], P('sp', 'tp'), may hold values from -0.125 to 0.125
- w_value: bfloat16 [2048, 2048], P('sp', 'tp'), may hold values from -0.125 to 0.125
- w_fwd_gate: bfloat16 [2048, 2048], P('sp', 'tp'), may hold values from -0.125 to 0.125
- w_bwd_gate: bfloat16 [2048, 2048], P('sp', 'tp'), may hold values from -0.125 to 0.125
- w_out_gate: bfloat16 [2048, 2048], P('sp', 'tp'), may hold values from -0.125 to 0.125
- floor_gap: float32 [2, 2048], P(None, 'tp'), may hold values from 0.00078125 to 0.1
- decay_shift: float32 [256, 8, 2048], P('sp', 'grp', 'tp'), parts along dimension 1, may hold values from -1.1 to 0
- head_gain: float32 [128], replicated, may hold values from 0.1 to 1.9
- w_out: bfloat16 [2048, 2048], P('tp', 'sp'), may hold values from -0.125 to 0.125
Outputs:
- layer_out: bfloat16 [256, 8, 2048], P(('sp', 'tp'), 'grp'), parts along dimension 1
The draws below stay inside these ranges and needn't reach their ends.
There are 2 independent parts, one for each index of `grp`. The reference program is written for one: setup_inputs(seed, part) draws one part's arguments, and reference() takes and returns one part's arrays. A program takes and returns all parts, laid end to end along the dimension named above; an argument that names none is the same for every part. Nothing has to cross between parts.
All inputs are finite; a program needn't handle non-finite values.
Results may differ from the reference program's by a relative error of at most 0.013.
Values may be sent and summed in bfloat16 or wider, within the bound.
A program may use at most 128 MiB of HBM per device.

```python
import math
import jax
import jax.numpy as jnp
from jax import lax

D = 2048
HEADS = 16
KEY = 128
VAL = 128
SEQS = 4
SPAN = 64
TOKENS = 256
N_TP = 4


def draw_floor_gap(key, part):
    key_order, key_count, key_slow, key_fast = jax.random.split(key, 4)
    head_ranks = jax.random.permutation(key_order, HEADS)
    slow_count = jax.random.randint(key_count, (), 2, HEADS - 1)
    slow_heads = jnp.repeat(head_ranks < slow_count, KEY)[None, :]
    slow_gap = jnp.exp(jax.random.uniform(key_slow, (2, HEADS * KEY), jnp.float32, math.log(0.2), math.log(0.8))) / TOKENS
    fast_gap = jnp.exp(jax.random.uniform(key_fast, (2, HEADS * KEY), jnp.float32, math.log(0.03), math.log(0.1)))
    return jnp.where(slow_heads, slow_gap, fast_gap).astype(jnp.float32)


def draw_decay_shift(key, part):
    key_block, key_chan, key_place, key_depth = jax.random.split(key, 4)
    block_rate = jnp.exp(jax.random.uniform(key_block, (TOKENS // SPAN, SEQS, 1), jnp.float32, math.log(0.5), math.log(2.0)))
    channel_rate = jnp.exp(jax.random.uniform(key_chan, (1, 1, HEADS * KEY), jnp.float32, math.log(0.3), 0.0))
    stable_regime = -(0.5 / TOKENS) * jnp.repeat(block_rate, SPAN, axis=0) * channel_rate
    seat_indices = jax.random.randint(key_place, (2, SEQS), 0, TOKENS)
    layer_tiers = jax.random.uniform(key_depth, (2, SEQS), jnp.float32, math.log(0.6), math.log(0.8))
    location_indices = jnp.arange(TOKENS)[:, None]
    cluster_tally = jnp.where(location_indices == seat_indices[0][None, :], layer_tiers[0][None, :], 0.0)
    cluster_tally = cluster_tally + jnp.where(location_indices == seat_indices[1][None, :], layer_tiers[1][None, :], 0.0)
    return (stable_regime + cluster_tally[:, :, None]).astype(jnp.float32)


def steps_of(key, extent, cuts, least, top_value):
    factor_of, own = 1.0, jax.random.fold_in(key, 6)
    for position, parts in cuts:
        draws = jnp.exp(jax.random.uniform(jax.random.fold_in(own, position), (parts,), jnp.float32, least / len(cuts), top_value / len(cuts)))
        factor_of = factor_of * jnp.repeat(draws, extent[position] // parts).reshape([-1 if axis == position else 1 for axis in range(len(extent))])
    return factor_of


def gaussian(stream_key, extent, deviation, reach, cuts=(), dtype=jnp.bfloat16):
    level = steps_of(stream_key, extent, cuts, -0.22, 0.18) if cuts else 1.0
    entries = jax.random.normal(stream_key, extent, jnp.float32) * deviation * level
    return jnp.minimum(jnp.maximum(entries, -reach), reach).astype(dtype)


def setup_inputs(seed: int = 0, part: int = 0) -> dict:
    splits = jax.random.split(jax.random.key(seed), 12)
    part_splits = jax.random.split(jax.random.fold_in(splits[11], part), 12)
    tokens = gaussian(part_splits[0], (TOKENS, SEQS, D), 1.0, 6.0, ((0, 16),))
    norm_gain = jnp.clip(1.0 + 0.18 * jax.random.normal(splits[1], (D,), jnp.float32), 0.1, 1.9)
    w_query = gaussian(splits[2], (D, HEADS * KEY), D ** -0.5, 0.125, ((0, 4), (1, 4)))
    w_value = gaussian(splits[3], (D, HEADS * VAL), D ** -0.5, 0.125, ((0, 4), (1, 4)))
    w_fwd_gate = gaussian(splits[4], (D, HEADS * KEY), D ** -0.5, 0.125, ((0, 4), (1, 4)))
    w_bwd_gate = gaussian(splits[5], (D, HEADS * KEY), D ** -0.5, 0.125, ((0, 4), (1, 4)))
    w_out_gate = gaussian(splits[6], (D, HEADS * VAL), D ** -0.5, 0.125, ((0, 4), (1, 4)))
    floor_gap = draw_floor_gap(jax.random.fold_in(splits[11], 71), part)
    decay_shift = draw_decay_shift(jax.random.fold_in(jax.random.fold_in(splits[11], part), 71), part)
    head_gain = jnp.clip(1.0 + 0.18 * jax.random.normal(splits[9], (VAL,), jnp.float32), 0.1, 1.9)
    w_out = gaussian(splits[10], (HEADS * VAL, D), (HEADS * VAL) ** -0.5, 0.125, ((0, 4), (1, 4)))
    return {"tokens": tokens, "norm_gain": norm_gain, "w_query": w_query, "w_value": w_value, "w_fwd_gate": w_fwd_gate, "w_bwd_gate": w_bwd_gate, "w_out_gate": w_out_gate, "floor_gap": floor_gap, "decay_shift": decay_shift, "head_gain": head_gain, "w_out": w_out}


norm_eps = 1e-06
highest = lax.Precision.HIGHEST

def chain_scan(queries, key_cols, values, log_decay, backward):

    def advance(carry_state, inputs):
        query_now, key_now, value_now, decay_now = inputs
        carry_state = jnp.exp(decay_now)[..., None] * carry_state + key_now[..., None] * value_now[..., None, :]
        return (carry_state, jnp.einsum('bhk,bhke->bhe', query_now, carry_state, precision=highest))
    start_state = jnp.zeros((SEQS, HEADS, KEY, VAL), jnp.float32)
    _, outputs = lax.scan(advance, start_state, (queries, key_cols, values, log_decay), reverse=backward)
    return outputs

def reference(tokens, norm_gain, w_query, w_value, w_fwd_gate, w_bwd_gate, w_out_gate, floor_gap, decay_shift, head_gain, w_out):
    token_f32 = tokens.astype(jnp.float32)
    scale_rows = lax.rsqrt(lax.optimization_barrier(jnp.mean(token_f32 * token_f32, axis=-1, keepdims=True)) + norm_eps)
    normed = (token_f32 * scale_rows * norm_gain.astype(jnp.float32)).astype(jnp.bfloat16)
    flat_rows = normed.reshape(TOKENS * SEQS, D)

    def project(matrix):
        rounded = jnp.dot(flat_rows, matrix, preferred_element_type=jnp.float32).astype(jnp.bfloat16)
        return lax.optimization_barrier(rounded).astype(jnp.float32)
    queries = jax.nn.silu(project(w_query)).reshape(TOKENS, SEQS, HEADS, KEY)
    values = project(w_value).reshape(TOKENS, SEQS, HEADS, VAL)
    shift = decay_shift.reshape(TOKENS, SEQS, HEADS, KEY)
    gap_fwd = floor_gap[0].reshape(HEADS, KEY)
    gap_bwd = floor_gap[1].reshape(HEADS, KEY)
    key_fwd = gap_fwd * jax.nn.sigmoid(-project(w_fwd_gate).reshape(TOKENS, SEQS, HEADS, KEY))
    key_bwd = gap_bwd * jax.nn.sigmoid(-project(w_bwd_gate).reshape(TOKENS, SEQS, HEADS, KEY))
    decay_fwd = jnp.log1p(-key_fwd) + shift
    decay_bwd = jnp.log1p(-key_bwd) + shift
    combined = chain_scan(queries, key_fwd, values, decay_fwd, False) + chain_scan(queries, key_bwd, values, decay_bwd, True)
    head_normed = combined * lax.rsqrt(lax.optimization_barrier(jnp.mean(combined * combined, axis=-1, keepdims=True)) + norm_eps) * head_gain.astype(jnp.float32)
    gate_value = jax.nn.silu(project(w_out_gate))
    mixed = (head_normed.reshape(TOKENS * SEQS, HEADS * VAL) * gate_value).astype(jnp.bfloat16)
    group_width = HEADS * VAL // N_TP
    accumulated_total = jnp.zeros((TOKENS * SEQS, D), jnp.float32)
    for tp_group in range(N_TP):
        first_column = tp_group * group_width
        partial_value = jnp.dot(mixed[:, first_column:first_column + group_width], w_out[first_column:first_column + group_width], preferred_element_type=jnp.float32).astype(jnp.bfloat16)
        accumulated_total = accumulated_total + lax.optimization_barrier(partial_value).astype(jnp.float32)
    return accumulated_total.astype(jnp.bfloat16).reshape(TOKENS, SEQS, D)
```

```python
import functools

import jax
import jax.numpy as jnp
from jax import lax
from jax.experimental import pallas as pl
from jax.experimental.pallas import tpu as pltpu
from jax.sharding import PartitionSpec as P

KEY = 128
VAL = 128
BLOCK = 64


norm_eps = 1e-06
highest = lax.Precision.HIGHEST


def carried_in(x, axis, join, neutral, backward):
    count = lax.axis_size(axis)
    place = lax.axis_index(axis)
    ahead = count - 1 - place if backward else place
    gathered = jax.tree.map(
        lambda a, kind: lax.all_gather(a.astype(kind), axis), x, (jnp.bfloat16, jnp.bfloat16)
    )
    state = jax.tree.map(lambda a, e: jnp.zeros_like(a) + jnp.asarray(e, a.dtype), x, neutral)

    def one(turn, state):
        source = count - 1 - turn if backward else turn
        return join(
            state,
            jax.tree.map(
                lambda a, own: lax.dynamic_index_in_dim(a, source, 0, False).astype(own.dtype),
                gathered,
                x,
            ),
        )

    return lax.fori_loop(0, ahead, one, state)


def split_blocks(array):
    return array.reshape(array.shape[0] // BLOCK, BLOCK, *array.shape[1:])


def prepare_chain(queries, key_cols, values, log_decay):
    query_blocks = split_blocks(queries)
    key_blocks = split_blocks(key_cols)
    value_blocks = split_blocks(values)
    running = jnp.cumsum(split_blocks(log_decay), axis=1)
    block_end = running[:, -1]
    block_state = jnp.einsum(
        "nsbhk,nsbhe->nbhke",
        key_blocks * jnp.exp(block_end[:, None] - running),
        value_blocks,
        precision=highest,
    )
    carry_state = jnp.zeros_like(block_state[0])
    log_total = jnp.zeros_like(block_end[0])
    offsets = [log_total]
    carry_state = jnp.exp(block_end[0])[..., None] * carry_state + block_state[0]
    log_total = block_end[0]
    return (
        query_blocks,
        key_blocks,
        value_blocks,
        running,
        block_state,
        jnp.stack(offsets),
        log_total,
        carry_state,
    )


def local_pass(chain, carry_state):
    query_blocks, key_blocks, value_blocks, running, block_state = (
        chain[0],
        chain[1],
        chain[2],
        chain[3],
        chain[4],
    )
    block_len = running.shape[1]
    earlier_mask = jnp.arange(block_len)[:, None] >= jnp.arange(block_len)[None, :]
    here = running[0]
    anchor = here[:1]
    query_scaled = query_blocks[0] * jnp.exp(here - anchor)
    key_scaled = key_blocks[0] * jnp.exp(anchor - here)
    scores = jnp.einsum("tbhk,sbhk->bhts", query_scaled, key_scaled, precision=highest)
    scores = jnp.where(earlier_mask, scores, 0.0)
    within = jnp.einsum("bhts,sbhe->tbhe", scores, value_blocks[0], precision=highest)
    carried = jnp.einsum(
        "tbhk,bhke->tbhe", query_blocks[0] * jnp.exp(here), carry_state, precision=highest
    )
    outputs = within + carried
    return outputs


def combine(earlier, later):
    return (earlier[0] + later[0], jnp.exp(later[0])[..., None] * earlier[1] + later[1])


def group_sums(flat_mixed, weight_lines, group_count):
    group_width = flat_mixed.shape[1] // group_count
    accumulated_total = jnp.zeros((flat_mixed.shape[0], weight_lines.shape[1]), jnp.float32)
    for tp_group in range(group_count):
        first_column = tp_group * group_width
        partial_value = jnp.dot(
            flat_mixed[:, first_column : first_column + group_width],
            weight_lines[first_column : first_column + group_width],
            preferred_element_type=jnp.float32,
        ).astype(jnp.bfloat16)
        accumulated_total = accumulated_total + lax.optimization_barrier(partial_value).astype(
            jnp.float32
        )
    return accumulated_total


def shards(
    tokens,
    norm_gain,
    w_query,
    w_value,
    w_fwd_gate,
    w_bwd_gate,
    w_out_gate,
    floor_gap,
    decay_shift,
    head_gain,
    w_out,
):
    token_f32 = tokens.astype(jnp.float32)
    scale_rows = lax.rsqrt(jnp.mean(token_f32 * token_f32, axis=-1, keepdims=True) + norm_eps)
    normed = (token_f32 * scale_rows * norm_gain).astype(jnp.bfloat16)
    weights = (
        lax.all_gather(w_query, "sp", axis=0, tiled=True),
        lax.all_gather(w_value, "sp", axis=0, tiled=True),
        lax.all_gather(w_fwd_gate, "sp", axis=0, tiled=True),
        lax.all_gather(w_bwd_gate, "sp", axis=0, tiled=True),
        lax.all_gather(w_out_gate, "sp", axis=0, tiled=True),
    )
    piece_rows = lax.all_gather(normed, "tp", axis=0, tiled=True)
    flat_rows = piece_rows.reshape(-1, piece_rows.shape[2])
    columns = [
        jnp.dot(flat_rows, matrix, preferred_element_type=jnp.float32).astype(jnp.bfloat16)
        for matrix in weights
    ]
    projected = lax.optimization_barrier(
        jnp.concatenate(columns, axis=1).reshape(piece_rows.shape[0], piece_rows.shape[1], -1)
    )
    key_width = w_query.shape[1]
    value_width = w_value.shape[1]
    heads_here = key_width // KEY
    extent_rows = projected.shape[0]
    seq_count = projected.shape[1]
    bounds_list = [
        0,
        key_width,
        key_width + value_width,
        2 * key_width + value_width,
        3 * key_width + value_width,
        3 * key_width + 2 * value_width,
    ]

    def section_part(position, feature_lanes):
        picked = projected[:, :, bounds_list[position] : bounds_list[position + 1]].astype(
            jnp.float32
        )
        return picked.reshape(extent_rows, seq_count, heads_here, feature_lanes)

    queries = jax.nn.silu(section_part(0, KEY))
    values = section_part(1, VAL)
    shift = decay_shift.reshape(extent_rows, seq_count, heads_here, KEY)
    key_fwd = floor_gap[0].reshape(heads_here, KEY) * jax.nn.sigmoid(-section_part(2, KEY))
    key_bwd = floor_gap[1].reshape(heads_here, KEY) * jax.nn.sigmoid(-section_part(3, KEY))
    decay_fwd = jnp.log1p(-key_fwd) + shift
    decay_bwd = jnp.log1p(-key_bwd) + shift
    fwd_chain = prepare_chain(queries, key_fwd, values, decay_fwd)
    bwd_chain = prepare_chain(queries[::-1], key_bwd[::-1], values[::-1], decay_bwd[::-1])
    identity_pair = (jnp.zeros_like(fwd_chain[6]), jnp.zeros_like(fwd_chain[7]))
    fwd_in = carried_in((fwd_chain[6], fwd_chain[7]), "sp", combine, identity_pair, False)[1]
    bwd_in = carried_in((bwd_chain[6], bwd_chain[7]), "sp", combine, identity_pair, True)[1]
    out_fwd = local_pass(fwd_chain, fwd_in)
    out_bwd = local_pass(bwd_chain, bwd_in)
    combined = out_fwd + out_bwd[::-1]
    head_normed = (
        combined
        * lax.rsqrt(jnp.mean(combined * combined, axis=-1, keepdims=True) + norm_eps)
        * head_gain
    )
    gate_value = jax.nn.silu(projected[:, :, bounds_list[4] : bounds_list[5]].astype(jnp.float32))
    mixed = (head_normed.reshape(extent_rows, seq_count, value_width) * gate_value).astype(
        jnp.bfloat16
    )
    token_rows = lax.all_to_all(mixed, "tp", split_axis=0, concat_axis=2, tiled=True)
    flat_mixed = token_rows.reshape(-1, token_rows.shape[2])
    group_count = lax.axis_size("tp")
    w_columns = lax.all_gather(w_out, "sp", axis=1, tiled=True)
    w_full = lax.all_gather(w_columns, "tp", axis=0, tiled=True)
    accumulated_total = group_sums(flat_mixed, w_full, group_count)
    result = accumulated_total.reshape(token_rows.shape[0], token_rows.shape[1], -1)
    return result.astype(jnp.bfloat16)


MESH = pl.DeviceIdType.MESH
CORES = 2


def greet(peers):
    barrier = pltpu.get_barrier_semaphore()
    for peer in peers:
        pl.semaphore_signal(barrier, inc=1, device_id=peer, device_id_type=MESH)
    pl.semaphore_wait(barrier, len(peers))


def gather_kernel(
    sizes,
    xn_ref,
    shift_ref,
    wq_ref,
    wv_ref,
    wf_ref,
    wb_ref,
    wg_ref,
    proj_ref,
    shift_out_ref,
    acts,
    weights,
    shifts,
    own_sem,
    az_sem,
    ax_sem,
    ac_sem,
    wz_sem,
    wy_sem,
    sz_sem,
):
    n_grp, n_sp, n_tp = sizes
    n_x = n_tp // CORES
    g = lax.axis_index("grp")
    s = lax.axis_index("sp")
    t = lax.axis_index("tp")
    x = t // CORES
    c = t % CORES
    seqs, span = xn_ref.shape[0], xn_ref.shape[1]
    depth = wq_ref.shape[0]
    part = depth // n_grp
    positions = shift_ref.shape[1]
    sources = (wq_ref, wv_ref, wf_ref, wb_ref, wg_ref)

    z_at = [s] + [lax.rem(s + k, n_sp) for k in range(1, n_sp)]
    z_from = [s] + [lax.rem(s + n_sp - k, n_sp) for k in range(1, n_sp)]
    x_at = [t] + [lax.rem(x + j, n_x) * CORES + c for j in range(1, n_x)]
    x_from = [t] + [lax.rem(x + n_x - j, n_x) * CORES + c for j in range(1, n_x)]
    twin = x * CORES + (1 - c)
    y_at = [g] + [lax.rem(g + m, n_grp) for m in range(1, n_grp)]
    y_from = [g] + [lax.rem(g + n_grp - m, n_grp) for m in range(1, n_grp)]

    peers = [(g, z_at[k], t) for k in range(1, n_sp)]
    peers += [(g, s, x_at[j]) for j in range(1, n_x)]
    peers += [(g, s, twin)]
    peers += [(y_at[m], s, t) for m in range(1, n_grp)]
    greet(peers)

    def block(where_s, where_t):
        return acts.at[:, pl.ds(pl.multiple_of((where_s * n_tp + where_t) * span, span), span), :]

    def remote(src, dst, sems, index, peer):
        return pltpu.make_async_remote_copy(
            src_ref=src,
            dst_ref=dst,
            send_sem=sems.at[(0, *index)],
            recv_sem=sems.at[(1, *index)],
            device_id=peer,
            device_id_type=MESH,
        )

    def rows(where_s, where_g):
        return pl.ds(pl.multiple_of(where_s * depth + where_g * part, part), part)

    def lanes(where):
        return pl.ds(pl.multiple_of(where * KEY, KEY), KEY)

    mine = [
        pltpu.make_async_copy(
            w.at[:, lanes(s)],
            weights.at[pl.ds(pl.multiple_of(s * depth, depth), depth), pl.ds(p * KEY, KEY)],
            own_sem.at[p],
        )
        for p, w in enumerate(sources)
    ]
    mine.append(pltpu.make_async_copy(xn_ref, block(s, t), own_sem.at[len(sources)]))
    mine.append(
        pltpu.make_async_copy(
            shift_ref.at[:, :, lanes(s)],
            shifts.at[:, pl.ds(pl.multiple_of(s * positions, positions), positions), :],
            own_sem.at[len(sources) + 1],
        )
    )

    sent = []

    def go(copy):
        copy.start()
        sent.append(copy)
        return copy

    act_z = {}
    act_x = {}
    for k in range(1, n_sp):
        act_z[k] = go(remote(xn_ref, block(s, t), az_sem, (k - 1,), (g, z_at[k], t)))
    for j in range(1, n_x):
        act_x[j, 0] = go(remote(xn_ref, block(s, t), ax_sem, (j - 1, 0), (g, s, x_at[j])))
    act_c = {}
    act_c[0, 0] = go(remote(xn_ref, block(s, t), ac_sem, (0, 0), (g, s, twin)))
    w_z = {}
    for k in range(1, n_sp):
        for p, w in enumerate(sources):
            w_z[k, p] = go(
                remote(
                    w.at[pl.ds(pl.multiple_of(g * part, part), part), lanes(z_at[k])],
                    weights.at[rows(s, g), pl.ds(p * KEY, KEY)],
                    wz_sem,
                    (k - 1, p),
                    (g, z_at[k], t),
                )
            )
    s_z = {}
    for k in range(1, n_sp):
        s_z[k] = go(
            remote(
                shift_ref.at[:, :, lanes(z_at[k])],
                shifts.at[:, pl.ds(pl.multiple_of(s * positions, positions), positions), :],
                sz_sem,
                (k - 1,),
                (g, z_at[k], t),
            )
        )
    for copy in mine:
        copy.start()

    for k in range(1, n_sp):
        act_z[k].wait_recv()
        here = block(z_from[k], t)
        for j in range(1, n_x):
            act_x[j, k] = go(remote(here, here, ax_sem, (j - 1, k), (g, s, x_at[j])))
        act_c[0, k] = go(remote(here, here, ac_sem, (0, k), (g, s, twin)))
    for k in range(n_sp):
        for j in range(1, n_x):
            act_x[j, k].wait_recv()
            here = block(z_from[k], x_from[j])
            act_c[j, k] = go(remote(here, here, ac_sem, (j, k), (g, s, twin)))
    w_y = {}
    for k in range(1, n_sp):
        for p in range(len(sources)):
            w_z[k, p].wait_recv()
            here = weights.at[rows(z_from[k], g), pl.ds(p * KEY, KEY)]
            for m in range(1, n_grp):
                w_y[m, k, p] = go(remote(here, here, wy_sem, (m - 1, k - 1, p), (y_at[m], s, t)))
    for copy in mine:
        copy.wait()
    for copy in act_c.values():
        copy.wait_recv()
    for copy in w_y.values():
        copy.wait_recv()

    def project(q, carry):
        proj_ref[q] = jnp.dot(
            acts[q], weights[...], preferred_element_type=jnp.float32
        ).astype(jnp.bfloat16)
        return carry

    lax.fori_loop(0, seqs, project, 0)
    for copy in s_z.values():
        copy.wait_recv()
    shift_out_ref[...] = shifts[...]
    for copy in sent:
        copy.wait_send()


def gather_project(sizes, xn, shift, sources):
    n_grp, n_sp, n_tp = sizes
    n_x = n_tp // CORES
    seqs, span, model = xn.shape
    length = n_sp * n_tp * span
    width = len(sources) * KEY
    dma = pltpu.SemaphoreType.DMA
    hbm = pl.BlockSpec(memory_space=pltpu.HBM)
    vmem = pl.BlockSpec(memory_space=pltpu.VMEM)
    return pl.pallas_call(
        functools.partial(gather_kernel, sizes),
        out_shape=(
            jax.ShapeDtypeStruct((seqs, length, width), jnp.bfloat16),
            jax.ShapeDtypeStruct((seqs, length, KEY), jnp.float32),
        ),
        in_specs=[hbm] * (2 + len(sources)),
        out_specs=(vmem, vmem),
        scratch_shapes=[
            pltpu.VMEM((seqs, length, model), jnp.bfloat16),
            pltpu.VMEM((model, width), jnp.bfloat16),
            pltpu.VMEM((seqs, length, KEY), jnp.float32),
            dma((len(sources) + 2,)),
            dma((2, n_sp - 1)),
            dma((2, max(n_x - 1, 1), n_sp)),
            dma((2, n_x, n_sp)),
            dma((2, n_sp - 1, len(sources))),
            dma((2, max(n_grp - 1, 1), n_sp - 1, len(sources))),
            dma((2, n_sp - 1)),
        ],
        compiler_params=pltpu.CompilerParams(
            collective_id=0, has_side_effects=True, vmem_limit_bytes=56 * 1024 * 1024
        ),
    )(xn, shift, *sources)


def recur_kernel(proj_ref, shift_ref, gap_ref, gain_ref, mixed_ref, out_ref):
    f32 = jnp.float32
    bf16 = jnp.bfloat16
    length = proj_ref.shape[1]

    def cols(p):
        return proj_ref[0, :, p * KEY : (p + 1) * KEY]

    queries = cols(0).astype(f32)
    queries = queries * jax.nn.sigmoid(queries)
    values = cols(1)
    shift = shift_ref[0]
    row = lax.broadcasted_iota(jnp.int32, (BLOCK, BLOCK), 0)
    col = lax.broadcasted_iota(jnp.int32, (BLOCK, BLOCK), 1)
    blocks = length // BLOCK
    for d in range(2):
        keys = gap_ref[d : d + 1, :] * jax.nn.sigmoid(-cols(2 + d).astype(f32))
        decay = jnp.log1p(-keys) + shift
        seen = (row >= col) if d == 0 else (row <= col)
        tri = jnp.where(seen, 1.0, 0.0).astype(f32)
        state = None
        for step in range(blocks):
            n = step if d == 0 else blocks - 1 - step
            at = slice(n * BLOCK, (n + 1) * BLOCK)
            q, k, v = queries[at], keys[at], values[at]
            here = jnp.dot(tri, decay[at], precision=highest, preferred_element_type=f32)
            edge = here[BLOCK - 1 : BLOCK] if d == 0 else here[0:1]
            anchor = here[BLOCK // 2 : BLOCK // 2 + 1]
            scores = lax.dot_general(
                (q * jnp.exp(here - anchor)).astype(bf16),
                (k * jnp.exp(anchor - here)).astype(bf16),
                (((1,), (1,)), ((), ())),
                preferred_element_type=f32,
            )
            scores = jnp.where(seen, scores, 0.0).astype(bf16)
            out = jnp.dot(scores, v, preferred_element_type=f32)
            if state is not None:
                out = out + lax.dot_general(
                    (q * jnp.exp(here)).astype(bf16),
                    state.astype(bf16),
                    (((1,), (1,)), ((), ())),
                    preferred_element_type=f32,
                )
            if d == 0:
                out_ref[at] = out
            else:
                out_ref[at] = out_ref[at] + out
            if step < blocks - 1:
                fresh = lax.dot_general(
                    v,
                    (k * jnp.exp(edge - here)).astype(bf16),
                    (((0,), (0,)), ((), ())),
                    preferred_element_type=f32,
                )
                state = fresh if state is None else state * jnp.exp(edge) + fresh
    combined = out_ref[...]
    normed = combined * lax.rsqrt(jnp.mean(combined * combined, axis=-1, keepdims=True) + norm_eps)
    gate = cols(4).astype(f32)
    mixed_ref[0] = (normed * gain_ref[...] * (gate * jax.nn.sigmoid(gate))).astype(bf16)


def recur(proj, shift, gap, gain):
    seqs, length, width = proj.shape
    return pl.pallas_call(
        recur_kernel,
        grid=(seqs,),
        out_shape=jax.ShapeDtypeStruct((seqs, length, VAL), jnp.bfloat16),
        in_specs=[
            pl.BlockSpec((1, length, width), lambda i: (i, 0, 0)),
            pl.BlockSpec((1, length, KEY), lambda i: (i, 0, 0)),
            pl.BlockSpec((2, KEY), lambda i: (0, 0)),
            pl.BlockSpec((1, VAL), lambda i: (0, 0)),
        ],
        out_specs=pl.BlockSpec((1, length, VAL), lambda i: (i, 0, 0)),
        scratch_shapes=[pltpu.VMEM((length, VAL), jnp.float32)],
    )(proj, shift, gap, gain)


def mix_kernel(sizes, mixed_ref, w_ref, out_ref, heads, partial, landed, own_sem, m_sem, p_sem):
    n_grp, n_sp, n_tp = sizes
    g = lax.axis_index("grp")
    s = lax.axis_index("sp")
    t = lax.axis_index("tp")
    seqs = mixed_ref.shape[0]
    span = out_ref.shape[1]
    width = w_ref.shape[1]
    z_at = [lax.rem(s + k, n_sp) for k in range(n_sp)]
    z_from = [lax.rem(s + n_sp - k, n_sp) for k in range(n_sp)]
    t_at = [lax.rem(t + j, n_tp) for j in range(n_tp)]
    t_from = [lax.rem(t + n_tp - j, n_tp) for j in range(n_tp)]
    others = [(k, j) for k in range(n_sp) for j in range(n_tp) if k or j]
    greet([(g, z_at[k], t_at[j]) for k, j in others])

    def lanes(where, size):
        return pl.ds(pl.multiple_of(where * size, size), size)

    own = pltpu.make_async_copy(mixed_ref, heads.at[:, :, lanes(s, VAL)], own_sem)
    own.start()
    moves = [
        pltpu.make_async_remote_copy(
            src_ref=mixed_ref,
            dst_ref=heads.at[:, :, lanes(s, VAL)],
            send_sem=m_sem.at[0, k - 1],
            recv_sem=m_sem.at[1, k - 1],
            device_id=(g, z_at[k], t),
            device_id_type=MESH,
        )
        for k in range(1, n_sp)
    ]
    for copy in moves:
        copy.start()
    own.wait()
    for copy in moves:
        copy.wait_recv()

    def multiply(q, carry):
        partial[q] = jnp.dot(
            heads[q], w_ref[...], preferred_element_type=jnp.float32
        ).astype(jnp.bfloat16)
        return carry

    lax.fori_loop(0, seqs, multiply, 0)

    def piece(where_s, where_t):
        return pl.ds(pl.multiple_of((where_s * n_tp + where_t) * span, span), span)

    sends = [
        pltpu.make_async_remote_copy(
            src_ref=partial.at[:, piece(z_at[k], t_at[j]), :],
            dst_ref=landed.at[t, :, :, lanes(s, width)],
            send_sem=p_sem.at[0, k, j],
            recv_sem=p_sem.at[1, k, j],
            device_id=(g, z_at[k], t_at[j]),
            device_id_type=MESH,
        )
        for k, j in others
    ]
    for copy in sends:
        copy.start()
    landed[t, :, :, lanes(s, width)] = partial[:, piece(s, t), :]
    for copy in sends:
        copy.wait_recv()
    total = landed[0].astype(jnp.float32)
    for j in range(1, n_tp):
        total = total + landed[j].astype(jnp.float32)
    out_ref[...] = total.astype(jnp.bfloat16)
    for copy in moves + sends:
        copy.wait_send()


def mix(sizes, mixed, w_out):
    n_grp, n_sp, n_tp = sizes
    seqs, length, _ = mixed.shape
    span = length // (n_sp * n_tp)
    depth, width = w_out.shape
    dma = pltpu.SemaphoreType.DMA
    vmem = pl.BlockSpec(memory_space=pltpu.VMEM)
    return pl.pallas_call(
        functools.partial(mix_kernel, sizes),
        out_shape=jax.ShapeDtypeStruct((seqs, span, n_sp * width), jnp.bfloat16),
        in_specs=[pl.BlockSpec(memory_space=pltpu.HBM), vmem],
        out_specs=vmem,
        scratch_shapes=[
            pltpu.VMEM((seqs, length, depth), jnp.bfloat16),
            pltpu.VMEM((seqs, length, width), jnp.bfloat16),
            pltpu.VMEM((n_tp, seqs, span, n_sp * width), jnp.bfloat16),
            dma,
            dma((2, n_sp - 1)),
            dma((2, n_sp, n_tp)),
        ],
        compiler_params=pltpu.CompilerParams(collective_id=1, has_side_effects=True),
    )(mixed, w_out)


def head_shards(
    sizes,
    tokens,
    norm_gain,
    w_query,
    w_value,
    w_fwd_gate,
    w_bwd_gate,
    w_out_gate,
    floor_gap,
    decay_shift,
    head_gain,
    w_out,
):
    token_f32 = tokens.astype(jnp.float32)
    scale_rows = lax.rsqrt(jnp.mean(token_f32 * token_f32, axis=-1, keepdims=True) + norm_eps)
    normed = (token_f32 * scale_rows * norm_gain).astype(jnp.bfloat16)
    proj, shift = gather_project(
        sizes,
        normed.transpose(1, 0, 2),
        decay_shift.transpose(1, 0, 2),
        (w_query, w_value, w_fwd_gate, w_bwd_gate, w_out_gate),
    )
    first = lax.axis_index("sp") * KEY
    gap = lax.dynamic_slice_in_dim(floor_gap, first, KEY, axis=1)
    mixed = recur(proj, shift, gap, head_gain.reshape(1, VAL))
    return mix(sizes, mixed, w_out).transpose(1, 0, 2)


def by_heads(mesh):
    n_sp, n_tp = mesh.shape["sp"], mesh.shape["tp"]

    def run(*arrays):
        tokens, w_query = arrays[0], arrays[2]
        heads_here = w_query.shape[1] // KEY // n_tp
        span = tokens.shape[0] // (n_sp * n_tp)
        sizes = (mesh.shape["grp"], n_sp, n_tp)
        fits = heads_here == n_sp and n_sp > 1 and n_tp % CORES == 0 and span % 16 == 0
        fits = fits and tokens.shape[0] % BLOCK == 0 and tokens.shape[0] <= 512
        body = functools.partial(head_shards, sizes) if fits else shards
        return mapped(body, mesh)(*arrays)

    return run


def mapped(body, mesh):
    return jax.shard_map(
        body,
        mesh=mesh,
        in_specs=(
            P(("sp", "tp"), "grp", None),
            P(),
            P("sp", "tp"),
            P("sp", "tp"),
            P("sp", "tp"),
            P("sp", "tp"),
            P("sp", "tp"),
            P(None, "tp"),
            P("sp", "grp", "tp"),
            P(),
            P("tp", "sp"),
        ),
        out_specs=P(("sp", "tp"), "grp", None),
        check_vma=False,
    )


def solution(mesh):
    return by_heads(mesh)
```

```python
import functools

import jax
import jax.numpy as jnp
from jax import lax
from jax.experimental import pallas as pl
from jax.experimental.pallas import tpu as pltpu
from jax.sharding import PartitionSpec as P

KEY = 128
VAL = 128
BLOCK = 64


norm_eps = 1e-06
highest = lax.Precision.HIGHEST


def carried_in(x, axis, join, neutral, backward):
    count = lax.axis_size(axis)
    place = lax.axis_index(axis)
    ahead = count - 1 - place if backward else place
    gathered = jax.tree.map(
        lambda a, kind: lax.all_gather(a.astype(kind), axis), x, (jnp.bfloat16, jnp.bfloat16)
    )
    state = jax.tree.map(lambda a, e: jnp.zeros_like(a) + jnp.asarray(e, a.dtype), x, neutral)

    def one(turn, state):
        source = count - 1 - turn if backward else turn
        return join(
            state,
            jax.tree.map(
                lambda a, own: lax.dynamic_index_in_dim(a, source, 0, False).astype(own.dtype),
                gathered,
                x,
            ),
        )

    return lax.fori_loop(0, ahead, one, state)


def split_blocks(array):
    return array.reshape(array.shape[0] // BLOCK, BLOCK, *array.shape[1:])


def prepare_chain(queries, key_cols, values, log_decay):
    query_blocks = split_blocks(queries)
    key_blocks = split_blocks(key_cols)
    value_blocks = split_blocks(values)
    running = jnp.cumsum(split_blocks(log_decay), axis=1)
    block_end = running[:, -1]
    block_state = jnp.einsum(
        "nsbhk,nsbhe->nbhke",
        key_blocks * jnp.exp(block_end[:, None] - running),
        value_blocks,
        precision=highest,
    )
    carry_state = jnp.zeros_like(block_state[0])
    log_total = jnp.zeros_like(block_end[0])
    offsets = [log_total]
    carry_state = jnp.exp(block_end[0])[..., None] * carry_state + block_state[0]
    log_total = block_end[0]
    return (
        query_blocks,
        key_blocks,
        value_blocks,
        running,
        block_state,
        jnp.stack(offsets),
        log_total,
        carry_state,
    )


def local_pass(chain, carry_state):
    query_blocks, key_blocks, value_blocks, running, block_state = (
        chain[0],
        chain[1],
        chain[2],
        chain[3],
        chain[4],
    )
    block_len = running.shape[1]
    earlier_mask = jnp.arange(block_len)[:, None] >= jnp.arange(block_len)[None, :]
    here = running[0]
    anchor = here[:1]
    query_scaled = query_blocks[0] * jnp.exp(here - anchor)
    key_scaled = key_blocks[0] * jnp.exp(anchor - here)
    scores = jnp.einsum("tbhk,sbhk->bhts", query_scaled, key_scaled, precision=highest)
    scores = jnp.where(earlier_mask, scores, 0.0)
    within = jnp.einsum("bhts,sbhe->tbhe", scores, value_blocks[0], precision=highest)
    carried = jnp.einsum(
        "tbhk,bhke->tbhe", query_blocks[0] * jnp.exp(here), carry_state, precision=highest
    )
    outputs = within + carried
    return outputs


def combine(earlier, later):
    return (earlier[0] + later[0], jnp.exp(later[0])[..., None] * earlier[1] + later[1])


def group_sums(flat_mixed, weight_lines, group_count):
    group_width = flat_mixed.shape[1] // group_count
    accumulated_total = jnp.zeros((flat_mixed.shape[0], weight_lines.shape[1]), jnp.float32)
    for tp_group in range(group_count):
        first_column = tp_group * group_width
        partial_value = jnp.dot(
            flat_mixed[:, first_column : first_column + group_width],
            weight_lines[first_column : first_column + group_width],
            preferred_element_type=jnp.float32,
        ).astype(jnp.bfloat16)
        accumulated_total = accumulated_total + lax.optimization_barrier(partial_value).astype(
            jnp.float32
        )
    return accumulated_total


def shards(
    tokens,
    norm_gain,
    w_query,
    w_value,
    w_fwd_gate,
    w_bwd_gate,
    w_out_gate,
    floor_gap,
    decay_shift,
    head_gain,
    w_out,
):
    token_f32 = tokens.astype(jnp.float32)
    scale_rows = lax.rsqrt(jnp.mean(token_f32 * token_f32, axis=-1, keepdims=True) + norm_eps)
    normed = (token_f32 * scale_rows * norm_gain).astype(jnp.bfloat16)
    weights = (
        lax.all_gather(w_query, "sp", axis=0, tiled=True),
        lax.all_gather(w_value, "sp", axis=0, tiled=True),
        lax.all_gather(w_fwd_gate, "sp", axis=0, tiled=True),
        lax.all_gather(w_bwd_gate, "sp", axis=0, tiled=True),
        lax.all_gather(w_out_gate, "sp", axis=0, tiled=True),
    )
    piece_rows = lax.all_gather(normed, "tp", axis=0, tiled=True)
    flat_rows = piece_rows.reshape(-1, piece_rows.shape[2])
    columns = [
        jnp.dot(flat_rows, matrix, preferred_element_type=jnp.float32).astype(jnp.bfloat16)
        for matrix in weights
    ]
    projected = lax.optimization_barrier(
        jnp.concatenate(columns, axis=1).reshape(piece_rows.shape[0], piece_rows.shape[1], -1)
    )
    key_width = w_query.shape[1]
    value_width = w_value.shape[1]
    heads_here = key_width // KEY
    extent_rows = projected.shape[0]
    seq_count = projected.shape[1]
    bounds_list = [
        0,
        key_width,
        key_width + value_width,
        2 * key_width + value_width,
        3 * key_width + value_width,
        3 * key_width + 2 * value_width,
    ]

    def section_part(position, feature_lanes):
        picked = projected[:, :, bounds_list[position] : bounds_list[position + 1]].astype(
            jnp.float32
        )
        return picked.reshape(extent_rows, seq_count, heads_here, feature_lanes)

    queries = jax.nn.silu(section_part(0, KEY))
    values = section_part(1, VAL)
    shift = decay_shift.reshape(extent_rows, seq_count, heads_here, KEY)
    key_fwd = floor_gap[0].reshape(heads_here, KEY) * jax.nn.sigmoid(-section_part(2, KEY))
    key_bwd = floor_gap[1].reshape(heads_here, KEY) * jax.nn.sigmoid(-section_part(3, KEY))
    decay_fwd = jnp.log1p(-key_fwd) + shift
    decay_bwd = jnp.log1p(-key_bwd) + shift
    fwd_chain = prepare_chain(queries, key_fwd, values, decay_fwd)
    bwd_chain = prepare_chain(queries[::-1], key_bwd[::-1], values[::-1], decay_bwd[::-1])
    identity_pair = (jnp.zeros_like(fwd_chain[6]), jnp.zeros_like(fwd_chain[7]))
    fwd_in = carried_in((fwd_chain[6], fwd_chain[7]), "sp", combine, identity_pair, False)[1]
    bwd_in = carried_in((bwd_chain[6], bwd_chain[7]), "sp", combine, identity_pair, True)[1]
    out_fwd = local_pass(fwd_chain, fwd_in)
    out_bwd = local_pass(bwd_chain, bwd_in)
    combined = out_fwd + out_bwd[::-1]
    head_normed = (
        combined
        * lax.rsqrt(jnp.mean(combined * combined, axis=-1, keepdims=True) + norm_eps)
        * head_gain
    )
    gate_value = jax.nn.silu(projected[:, :, bounds_list[4] : bounds_list[5]].astype(jnp.float32))
    mixed = (head_normed.reshape(extent_rows, seq_count, value_width) * gate_value).astype(
        jnp.bfloat16
    )
    token_rows = lax.all_to_all(mixed, "tp", split_axis=0, concat_axis=2, tiled=True)
    flat_mixed = token_rows.reshape(-1, token_rows.shape[2])
    group_count = lax.axis_size("tp")
    w_columns = lax.all_gather(w_out, "sp", axis=1, tiled=True)
    w_full = lax.all_gather(w_columns, "tp", axis=0, tiled=True)
    accumulated_total = group_sums(flat_mixed, w_full, group_count)
    result = accumulated_total.reshape(token_rows.shape[0], token_rows.shape[1], -1)
    return result.astype(jnp.bfloat16)


MESH = pl.DeviceIdType.MESH
CORES = 2


def greet(peers):
    barrier = pltpu.get_barrier_semaphore()
    for peer in peers:
        pl.semaphore_signal(barrier, inc=1, device_id=peer, device_id_type=MESH)
    pl.semaphore_wait(barrier, len(peers))


def gather_kernel(
    sizes,
    xn_ref,
    shift_ref,
    wq_ref,
    wv_ref,
    wf_ref,
    wb_ref,
    wg_ref,
    proj_ref,
    shift_out_ref,
    acts,
    weights,
    shifts,
    own_sem,
    az_sem,
    ax_sem,
    ac_sem,
    wz_sem,
    wy_sem,
    sz_sem,
):
    n_grp, n_sp, n_tp = sizes
    n_x = n_tp // CORES
    g = lax.axis_index("grp")
    s = lax.axis_index("sp")
    t = lax.axis_index("tp")
    x = t // CORES
    c = t % CORES
    seqs, span = xn_ref.shape[0], xn_ref.shape[1]
    depth = wq_ref.shape[0]
    part = depth // n_grp
    positions = shift_ref.shape[1]
    sources = (wq_ref, wv_ref, wf_ref, wb_ref, wg_ref)

    z_at = [s] + [lax.rem(s + k, n_sp) for k in range(1, n_sp)]
    z_from = [s] + [lax.rem(s + n_sp - k, n_sp) for k in range(1, n_sp)]
    x_at = [t] + [lax.rem(x + j, n_x) * CORES + c for j in range(1, n_x)]
    x_from = [t] + [lax.rem(x + n_x - j, n_x) * CORES + c for j in range(1, n_x)]
    twin = x * CORES + (1 - c)
    y_at = [g] + [lax.rem(g + m, n_grp) for m in range(1, n_grp)]
    y_from = [g] + [lax.rem(g + n_grp - m, n_grp) for m in range(1, n_grp)]

    peers = [(g, z_at[k], t) for k in range(1, n_sp)]
    peers += [(g, s, x_at[j]) for j in range(1, n_x)]
    peers += [(g, s, twin)]
    peers += [(y_at[m], s, t) for m in range(1, n_grp)]
    greet(peers)

    def block(where_s, where_t):
        return acts.at[:, pl.ds(pl.multiple_of((where_s * n_tp + where_t) * span, span), span), :]

    def remote(src, dst, sems, index, peer):
        return pltpu.make_async_remote_copy(
            src_ref=src,
            dst_ref=dst,
            send_sem=sems.at[(0, *index)],
            recv_sem=sems.at[(1, *index)],
            device_id=peer,
            device_id_type=MESH,
        )

    def rows(where_s, where_g):
        return pl.ds(pl.multiple_of(where_s * depth + where_g * part, part), part)

    def lanes(where):
        return pl.ds(pl.multiple_of(where * KEY, KEY), KEY)

    mine = [
        pltpu.make_async_copy(
            w.at[:, lanes(s)],
            weights.at[pl.ds(pl.multiple_of(s * depth, depth), depth), pl.ds(p * KEY, KEY)],
            own_sem.at[p],
        )
        for p, w in enumerate(sources)
    ]
    mine.append(pltpu.make_async_copy(xn_ref, block(s, t), own_sem.at[len(sources)]))
    mine.append(
        pltpu.make_async_copy(
            shift_ref.at[:, :, lanes(s)],
            shifts.at[:, pl.ds(pl.multiple_of(s * positions, positions), positions), :],
            own_sem.at[len(sources) + 1],
        )
    )

    sent = []

    def go(copy):
        copy.start()
        sent.append(copy)
        return copy

    def slot(up, d):
        return 1 + d if up else n_sp + d

    def chain(up, d):
        step = -1 if up else 1
        there = s - step
        sends = jnp.logical_and(
            jnp.logical_and(there >= 0, there < n_sp),
            jnp.logical_and(s + step * d >= 0, s + step * d < n_sp),
        )
        gets = jnp.logical_and(s + step * (d + 1) >= 0, s + step * (d + 1) < n_sp)
        return there, s + step * d, sends, s + step * (d + 1), gets

    def act_move(up, d, from_own):
        there, origin, _, _, _ = chain(up, d)
        src = xn_ref if from_own else block(origin, t)
        return remote(src, block(origin, t), az_sem, (slot(up, d) - 1,), (g, there, t))

    def act_spread(kind, j, index, where_s, where_t, from_own):
        src = xn_ref if from_own else block(where_s, where_t)
        if kind == "x":
            return remote(src, block(where_s, where_t), ax_sem, (j - 1, index), (g, s, x_at[j]))
        return remote(src, block(where_s, where_t), ac_sem, (j, index), (g, s, twin))

    for up in (True, False):
        _, _, sends, _, _ = chain(up, 0)

        @pl.when(sends)
        def _():
            act_move(up, 0, True).start()

    for j in range(1, n_x):
        act_spread("x", j, 0, s, t, True).start()
    act_spread("c", 0, 0, s, t, True).start()
    for copy in mine:
        copy.start()

    w_z = {}

    def send_weights(p):
        for k in range(1, n_sp):
            w_z[k, p] = go(
                remote(
                    sources[p].at[pl.ds(pl.multiple_of(g * part, part), part), lanes(z_at[k])],
                    weights.at[rows(s, g), pl.ds(p * KEY, KEY)],
                    wz_sem,
                    (k - 1, p),
                    (g, z_at[k], t),
                )
            )

    queue = list(range(len(sources)))
    for d in range(n_sp - 1):
        if queue:
            send_weights(queue.pop(0))
        for up in (True, False):
            _, _, _, origin, gets = chain(up, d)

            @pl.when(gets)
            def _():
                act_move(up, d, False).wait_recv()
                if d + 1 < n_sp - 1:
                    _, _, sends, _, _ = chain(up, d + 1)

                    @pl.when(sends)
                    def _():
                        act_move(up, d + 1, False).start()

                for j in range(1, n_x):
                    act_spread("x", j, slot(up, d), origin, t, False).start()
                act_spread("c", 0, slot(up, d), origin, t, False).start()

    for p in queue:
        send_weights(p)
    s_z = {}
    for k in range(1, n_sp):
        s_z[k] = go(
            remote(
                shift_ref.at[:, :, lanes(z_at[k])],
                shifts.at[:, pl.ds(pl.multiple_of(s * positions, positions), positions), :],
                sz_sem,
                (k - 1,),
                (g, z_at[k], t),
            )
        )

    def each_block(visit):
        visit(0, s)
        for d in range(n_sp - 1):
            for up in (True, False):
                _, _, _, origin, gets = chain(up, d)

                @pl.when(gets)
                def _():
                    visit(slot(up, d), origin)

    def relay(index, origin):
        for j in range(1, n_x):
            act_spread("x", j, index, origin, t, False).wait_recv()
            act_spread("c", j, index, origin, x_from[j], False).start()

    each_block(relay)
    w_y = {}
    for p in range(len(sources)):
        for k in range(1, n_sp):
            w_z[k, p].wait_recv()
            here = weights.at[rows(z_from[k], g), pl.ds(p * KEY, KEY)]
            for m in range(1, n_grp):
                w_y[m, k, p] = go(remote(here, here, wy_sem, (m - 1, k - 1, p), (y_at[m], s, t)))
    for copy in mine:
        copy.wait()

    def joined(index, origin):
        for j in range(n_x):
            act_spread("c", j, index, origin, t, False).wait_recv()

    each_block(joined)
    for first in range(0, len(sources), 2):
        last = min(first + 2, len(sources))
        for (m, k, p), copy in w_y.items():
            if first <= p < last:
                copy.wait_recv()
        at = slice(first * KEY, last * KEY)

        def project(q, carry):
            proj_ref[q, :, at] = jnp.dot(
                acts[q], weights[:, at], preferred_element_type=jnp.float32
            ).astype(jnp.bfloat16)
            return carry

        lax.fori_loop(0, seqs, project, 0)
    for copy in s_z.values():
        copy.wait_recv()
    shift_out_ref[...] = shifts[...]
    for d in range(n_sp - 1):
        for up in (True, False):
            _, _, sends, _, _ = chain(up, d)

            @pl.when(sends)
            def _():
                act_move(up, d, d == 0).wait_send()

    def gone(index, origin):
        for j in range(1, n_x):
            act_spread("x", j, index, origin, t, False).wait_send()
        for j in range(n_x):
            act_spread("c", j, index, origin, x_from[j], False).wait_send()

    each_block(gone)
    for copy in sent:
        copy.wait_send()


def gather_project(sizes, xn, shift, sources):
    n_grp, n_sp, n_tp = sizes
    n_x = n_tp // CORES
    seqs, span, model = xn.shape
    length = n_sp * n_tp * span
    width = len(sources) * KEY
    dma = pltpu.SemaphoreType.DMA
    hbm = pl.BlockSpec(memory_space=pltpu.HBM)
    vmem = pl.BlockSpec(memory_space=pltpu.VMEM)
    return pl.pallas_call(
        functools.partial(gather_kernel, sizes),
        out_shape=(
            jax.ShapeDtypeStruct((seqs, length, width), jnp.bfloat16),
            jax.ShapeDtypeStruct((seqs, length, KEY), shift.dtype),
        ),
        in_specs=[hbm] * (2 + len(sources)),
        out_specs=(vmem, vmem),
        scratch_shapes=[
            pltpu.VMEM((seqs, length, model), jnp.bfloat16),
            pltpu.VMEM((model, width), jnp.bfloat16),
            pltpu.VMEM((seqs, length, KEY), shift.dtype),
            dma((len(sources) + 2,)),
            dma((2, 2 * n_sp - 2)),
            dma((2, max(n_x - 1, 1), 2 * n_sp - 1)),
            dma((2, n_x, 2 * n_sp - 1)),
            dma((2, n_sp - 1, len(sources))),
            dma((2, max(n_grp - 1, 1), n_sp - 1, len(sources))),
            dma((2, n_sp - 1)),
        ],
        compiler_params=pltpu.CompilerParams(
            collective_id=0, has_side_effects=True, vmem_limit_bytes=56 * 1024 * 1024
        ),
    )(xn, shift, *sources)


def recur_one(proj_ref, shift_ref, gap_ref, gain_ref, out_ref, i):
    f32 = jnp.float32
    bf16 = jnp.bfloat16
    length = proj_ref.shape[1]

    def cols(p):
        return proj_ref[i, :, p * KEY : (p + 1) * KEY]

    queries = cols(0).astype(f32)
    queries = queries * jax.nn.sigmoid(queries)
    values = cols(1)
    shift = shift_ref[i].astype(f32)
    row = lax.broadcasted_iota(jnp.int32, (BLOCK, BLOCK), 0)
    col = lax.broadcasted_iota(jnp.int32, (BLOCK, BLOCK), 1)
    blocks = length // BLOCK
    for d in range(2):
        keys = gap_ref[d : d + 1, :] * jax.nn.sigmoid(-cols(2 + d).astype(f32))
        decay = jnp.log1p(-keys) + shift
        seen = (row >= col) if d == 0 else (row <= col)
        tri = jnp.where(seen, 1.0, 0.0).astype(f32)
        state = None
        for step in range(blocks):
            n = step if d == 0 else blocks - 1 - step
            at = slice(n * BLOCK, (n + 1) * BLOCK)
            q, k, v = queries[at], keys[at], values[at]
            here = jnp.dot(tri, decay[at], precision=highest, preferred_element_type=f32)
            edge = here[BLOCK - 1 : BLOCK] if d == 0 else here[0:1]
            anchor = here[BLOCK // 2 : BLOCK // 2 + 1]
            scores = lax.dot_general(
                (q * jnp.exp(here - anchor)).astype(bf16),
                (k * jnp.exp(anchor - here)).astype(bf16),
                (((1,), (1,)), ((), ())),
                preferred_element_type=f32,
            )
            scores = jnp.where(seen, scores, 0.0).astype(bf16)
            out = jnp.dot(scores, v, preferred_element_type=f32)
            if state is not None:
                out = out + lax.dot_general(
                    (q * jnp.exp(here)).astype(bf16),
                    state.astype(bf16),
                    (((1,), (1,)), ((), ())),
                    preferred_element_type=f32,
                )
            if d == 0:
                out_ref[at] = out
            else:
                out_ref[at] = out_ref[at] + out
            if step < blocks - 1:
                fresh = lax.dot_general(
                    v,
                    (k * jnp.exp(edge - here)).astype(bf16),
                    (((0,), (0,)), ((), ())),
                    preferred_element_type=f32,
                )
                state = fresh if state is None else state * jnp.exp(edge) + fresh
    combined = out_ref[...]
    normed = combined * lax.rsqrt(jnp.mean(combined * combined, axis=-1, keepdims=True) + norm_eps)
    gate = cols(4).astype(f32)
    return (normed * gain_ref[...] * (gate * jax.nn.sigmoid(gate))).astype(bf16)


def mix_kernel(
    sizes,
    proj_ref,
    shift_ref,
    gap_ref,
    gain_ref,
    w_ref,
    out_ref,
    summed,
    heads,
    matrix,
    partial,
    landed,
    own_sem,
    w_sem,
    z_sem,
    c_sem,
    p_sem,
):
    n_grp, n_sp, n_tp = sizes
    n_x = n_tp // CORES
    g = lax.axis_index("grp")
    s = lax.axis_index("sp")
    t = lax.axis_index("tp")
    x = t // CORES
    c = t % CORES
    twin = x * CORES + (1 - c)
    seqs = proj_ref.shape[0]
    span = out_ref.shape[1]
    depth, width = w_ref.shape[0], w_ref.shape[1] // CORES
    half = seqs // 2
    z_at = [lax.rem(s + k, n_sp) for k in range(n_sp)]
    t_at = [lax.rem(t + j, n_tp) for j in range(n_tp)]
    others = [(k, j) for k in range(n_sp) for j in range(n_tp) if k or j]
    greet([(g, z_at[k], t_at[j]) for k, j in others])

    def lanes(where, size):
        return pl.ds(pl.multiple_of(where * size, size), size)

    def remote(src, dst, sems, index, peer):
        return pltpu.make_async_remote_copy(
            src_ref=src,
            dst_ref=dst,
            send_sem=sems.at[(0, *index)],
            recv_sem=sems.at[(1, *index)],
            device_id=peer,
            device_id_type=MESH,
        )

    w_rows = pl.ds(pl.multiple_of(c * depth, depth), depth)
    w_own = pltpu.make_async_copy(w_ref.at[:, lanes(c, width)], matrix.at[w_rows, :], own_sem)
    w_twin = remote(w_ref.at[:, lanes(1 - c, width)], matrix.at[w_rows, :], w_sem, (), (g, s, twin))
    w_own.start()
    w_twin.start()

    def head(q, where):
        return heads.at[q, :, lanes(c * n_sp + where, VAL)]

    def slot(up, d):
        return 1 + d if up else n_sp + d

    def inside(place):
        return jnp.logical_and(place >= 0, place < n_sp)

    def z_move(q, up, d):
        step = 1 if up else -1
        here = head(q, s - step * d)
        return remote(here, here, z_sem, (q, slot(up, d) - 1), (g, s + step, t))

    def z_sends(up, d):
        step = 1 if up else -1
        return jnp.logical_and(inside(s + step), inside(s - step * d))

    def z_gets(up, d):
        step = 1 if up else -1
        return inside(s - step * (d + 1))

    def c_move(q, index, origin):
        here = head(q, origin)
        return remote(here, here, c_sem, (q, index), (g, s, twin))

    def each(d, visit):
        for up in (True, False):

            @pl.when(z_gets(up, d))
            def _():
                visit(up, s - (d + 1) if up else s + (d + 1))

    def arrived(q, d):
        def visit(up, origin):
            z_move(q, up, d).wait_recv()
            if d + 1 < n_sp - 1:

                @pl.when(z_sends(up, d + 1))
                def _():
                    z_move(q, up, d + 1).start()

            c_move(q, slot(up, d), origin).start()

        each(d, visit)

    def advance(q, carry):
        heads[q, :, lanes(c * n_sp + s, VAL)] = recur_one(
            proj_ref, shift_ref, gap_ref, gain_ref, summed, q
        )
        for up in (True, False):

            @pl.when(z_sends(up, 0))
            def _():
                z_move(q, up, 0).start()

        c_move(q, 0, s).start()
        for d in range(n_sp - 1):

            @pl.when(q >= d + 1)
            def _():
                arrived(q - (d + 1), d)

        return carry

    lax.fori_loop(0, seqs, advance, 0)

    def piece(where_s, where_t):
        return pl.ds(pl.multiple_of((where_s * n_tp + where_t) * span, span), span)

    def p_move(h, k, j):
        both = pl.ds(h * half, half)
        return remote(
            partial.at[both, piece(z_at[k], t_at[j]), :],
            landed.at[x, both, :, lanes(s * CORES + c, width)],
            p_sem,
            (h, k, j),
            (g, z_at[k], t_at[j]),
        )

    def finish(h):
        def one(q, carry):
            c_move(q, 0, s).wait_recv()
            for d in range(n_sp - 1):
                each(d, lambda up, origin: c_move(q, slot(up, d), origin).wait_recv())
            partial[q] = jnp.dot(
                heads[q], matrix[...], preferred_element_type=jnp.float32
            ).astype(jnp.bfloat16)
            return carry

        lax.fori_loop(h * half, (h + 1) * half, one, 0)
        for k, j in others:
            p_move(h, k, j).start()
        both = pl.ds(h * half, half)
        landed[x, both, :, lanes(s * CORES + c, width)] = partial[both, piece(s, t), :]

    w_own.wait()
    w_twin.wait_recv()
    pending = [
        (i - 1 - d, d)
        for i in range(seqs, seqs + n_sp - 1)
        for d in range(n_sp - 1)
        if 0 <= i - 1 - d < seqs
    ]
    early = [item for item in pending if item[0] < half]
    late = [item for item in pending if item[0] >= half]
    cut = pending.index(early[-1]) + 1 if early else 0
    for q, d in pending[:cut]:
        arrived(q, d)
    finish(0)
    for q, d in pending[cut:]:
        arrived(q, d)
    finish(1)
    for h in range(2):
        for k, j in others:
            p_move(h, k, j).wait_recv()
    total = landed[0].astype(jnp.float32)
    for j in range(1, n_x):
        total = total + landed[j].astype(jnp.float32)
    out_ref[...] = total.astype(jnp.bfloat16)

    w_twin.wait_send()

    def drain(q, carry):
        c_move(q, 0, s).wait_send()
        for d in range(n_sp - 1):
            each(d, lambda up, origin: c_move(q, slot(up, d), origin).wait_send())
            for up in (True, False):

                @pl.when(z_sends(up, d))
                def _():
                    z_move(q, up, d).wait_send()

        return carry

    lax.fori_loop(0, seqs, drain, 0)
    for h in range(2):
        for k, j in others:
            p_move(h, k, j).wait_send()


def mix(sizes, proj, shift, gap, gain, w_out):
    n_grp, n_sp, n_tp = sizes
    seqs, length, _ = proj.shape
    span = length // (n_sp * n_tp)
    depth, width = w_out.shape
    part = width // CORES
    dma = pltpu.SemaphoreType.DMA
    vmem = pl.BlockSpec(memory_space=pltpu.VMEM)
    return pl.pallas_call(
        functools.partial(mix_kernel, sizes),
        out_shape=jax.ShapeDtypeStruct((seqs, span, n_sp * width), jnp.bfloat16),
        in_specs=[vmem, vmem, vmem, vmem, pl.BlockSpec(memory_space=pltpu.HBM)],
        out_specs=vmem,
        scratch_shapes=[
            pltpu.VMEM((length, VAL), jnp.float32),
            pltpu.VMEM((seqs, length, CORES * depth), jnp.bfloat16),
            pltpu.VMEM((CORES * depth, part), jnp.bfloat16),
            pltpu.VMEM((seqs, length, part), jnp.bfloat16),
            pltpu.VMEM((n_tp // CORES, seqs, span, n_sp * width), jnp.bfloat16),
            dma,
            dma((2,)),
            dma((2, seqs, 2 * n_sp - 2)),
            dma((2, seqs, 2 * n_sp - 1)),
            dma((2, 2, n_sp, n_tp)),
        ],
        compiler_params=pltpu.CompilerParams(collective_id=1, has_side_effects=True),
    )(proj, shift, gap, gain, w_out)


def head_shards(
    sizes,
    tokens,
    norm_gain,
    w_query,
    w_value,
    w_fwd_gate,
    w_bwd_gate,
    w_out_gate,
    floor_gap,
    decay_shift,
    head_gain,
    w_out,
):
    token_f32 = tokens.astype(jnp.float32)
    scale_rows = lax.rsqrt(jnp.mean(token_f32 * token_f32, axis=-1, keepdims=True) + norm_eps)
    normed = (token_f32 * scale_rows * norm_gain).astype(jnp.bfloat16)
    proj, shift = gather_project(
        sizes,
        normed.transpose(1, 0, 2),
        decay_shift.astype(jnp.bfloat16).transpose(1, 0, 2),
        (w_query, w_value, w_fwd_gate, w_bwd_gate, w_out_gate),
    )
    first = lax.axis_index("sp") * KEY
    gap = lax.dynamic_slice_in_dim(floor_gap, first, KEY, axis=1)
    return mix(sizes, proj, shift, gap, head_gain.reshape(1, VAL), w_out).transpose(1, 0, 2)


def by_heads(mesh):
    n_sp, n_tp = mesh.shape["sp"], mesh.shape["tp"]

    def run(*arrays):
        tokens, w_query = arrays[0], arrays[2]
        heads_here = w_query.shape[1] // KEY // n_tp
        span = tokens.shape[0] // (n_sp * n_tp)
        sizes = (mesh.shape["grp"], n_sp, n_tp)
        fits = heads_here == n_sp and n_sp > 1 and n_tp % CORES == 0 and span % 16 == 0
        fits = fits and tokens.shape[1] // sizes[0] % 2 == 0
        fits = fits and tokens.shape[0] % BLOCK == 0 and tokens.shape[0] <= 512
        body = functools.partial(head_shards, sizes) if fits else shards
        return mapped(body, mesh)(*arrays)

    return run


def mapped(body, mesh):
    return jax.shard_map(
        body,
        mesh=mesh,
        in_specs=(
            P(("sp", "tp"), "grp", None),
            P(),
            P("sp", "tp"),
            P("sp", "tp"),
            P("sp", "tp"),
            P("sp", "tp"),
            P("sp", "tp"),
            P(None, "tp"),
            P("sp", "grp", "tp"),
            P(),
            P("tp", "sp"),
        ),
        out_specs=P(("sp", "tp"), "grp", None),
        check_vma=False,
    )


def solution(mesh):
    return by_heads(mesh)
```

```python
import functools

import jax
import jax.numpy as jnp
from jax import lax
from jax.experimental import pallas as pl
from jax.experimental.pallas import tpu as pltpu
from jax.sharding import PartitionSpec as P

KEY = 128
VAL = 128
BLOCK = 64


norm_eps = 1e-06
highest = lax.Precision.HIGHEST


def carried_in(x, axis, join, neutral, backward):
    count = lax.axis_size(axis)
    place = lax.axis_index(axis)
    ahead = count - 1 - place if backward else place
    gathered = jax.tree.map(
        lambda a, kind: lax.all_gather(a.astype(kind), axis), x, (jnp.bfloat16, jnp.bfloat16)
    )
    state = jax.tree.map(lambda a, e: jnp.zeros_like(a) + jnp.asarray(e, a.dtype), x, neutral)

    def one(turn, state):
        source = count - 1 - turn if backward else turn
        return join(
            state,
            jax.tree.map(
                lambda a, own: lax.dynamic_index_in_dim(a, source, 0, False).astype(own.dtype),
                gathered,
                x,
            ),
        )

    return lax.fori_loop(0, ahead, one, state)


def split_blocks(array):
    return array.reshape(array.shape[0] // BLOCK, BLOCK, *array.shape[1:])


def prepare_chain(queries, key_cols, values, log_decay):
    query_blocks = split_blocks(queries)
    key_blocks = split_blocks(key_cols)
    value_blocks = split_blocks(values)
    running = jnp.cumsum(split_blocks(log_decay), axis=1)
    block_end = running[:, -1]
    block_state = jnp.einsum(
        "nsbhk,nsbhe->nbhke",
        key_blocks * jnp.exp(block_end[:, None] - running),
        value_blocks,
        precision=highest,
    )
    carry_state = jnp.zeros_like(block_state[0])
    log_total = jnp.zeros_like(block_end[0])
    offsets = [log_total]
    carry_state = jnp.exp(block_end[0])[..., None] * carry_state + block_state[0]
    log_total = block_end[0]
    return (
        query_blocks,
        key_blocks,
        value_blocks,
        running,
        block_state,
        jnp.stack(offsets),
        log_total,
        carry_state,
    )


def local_pass(chain, carry_state):
    query_blocks, key_blocks, value_blocks, running, block_state = (
        chain[0],
        chain[1],
        chain[2],
        chain[3],
        chain[4],
    )
    block_len = running.shape[1]
    earlier_mask = jnp.arange(block_len)[:, None] >= jnp.arange(block_len)[None, :]
    here = running[0]
    anchor = here[:1]
    query_scaled = query_blocks[0] * jnp.exp(here - anchor)
    key_scaled = key_blocks[0] * jnp.exp(anchor - here)
    scores = jnp.einsum("tbhk,sbhk->bhts", query_scaled, key_scaled, precision=highest)
    scores = jnp.where(earlier_mask, scores, 0.0)
    within = jnp.einsum("bhts,sbhe->tbhe", scores, value_blocks[0], precision=highest)
    carried = jnp.einsum(
        "tbhk,bhke->tbhe", query_blocks[0] * jnp.exp(here), carry_state, precision=highest
    )
    outputs = within + carried
    return outputs


def combine(earlier, later):
    return (earlier[0] + later[0], jnp.exp(later[0])[..., None] * earlier[1] + later[1])


def group_sums(flat_mixed, weight_lines, group_count):
    group_width = flat_mixed.shape[1] // group_count
    accumulated_total = jnp.zeros((flat_mixed.shape[0], weight_lines.shape[1]), jnp.float32)
    for tp_group in range(group_count):
        first_column = tp_group * group_width
        partial_value = jnp.dot(
            flat_mixed[:, first_column : first_column + group_width],
            weight_lines[first_column : first_column + group_width],
            preferred_element_type=jnp.float32,
        ).astype(jnp.bfloat16)
        accumulated_total = accumulated_total + lax.optimization_barrier(partial_value).astype(
            jnp.float32
        )
    return accumulated_total


def shards(
    tokens,
    norm_gain,
    w_query,
    w_value,
    w_fwd_gate,
    w_bwd_gate,
    w_out_gate,
    floor_gap,
    decay_shift,
    head_gain,
    w_out,
):
    token_f32 = tokens.astype(jnp.float32)
    scale_rows = lax.rsqrt(jnp.mean(token_f32 * token_f32, axis=-1, keepdims=True) + norm_eps)
    normed = (token_f32 * scale_rows * norm_gain).astype(jnp.bfloat16)
    weights = (
        lax.all_gather(w_query, "sp", axis=0, tiled=True),
        lax.all_gather(w_value, "sp", axis=0, tiled=True),
        lax.all_gather(w_fwd_gate, "sp", axis=0, tiled=True),
        lax.all_gather(w_bwd_gate, "sp", axis=0, tiled=True),
        lax.all_gather(w_out_gate, "sp", axis=0, tiled=True),
    )
    piece_rows = lax.all_gather(normed, "tp", axis=0, tiled=True)
    flat_rows = piece_rows.reshape(-1, piece_rows.shape[2])
    columns = [
        jnp.dot(flat_rows, matrix, preferred_element_type=jnp.float32).astype(jnp.bfloat16)
        for matrix in weights
    ]
    projected = lax.optimization_barrier(
        jnp.concatenate(columns, axis=1).reshape(piece_rows.shape[0], piece_rows.shape[1], -1)
    )
    key_width = w_query.shape[1]
    value_width = w_value.shape[1]
    heads_here = key_width // KEY
    extent_rows = projected.shape[0]
    seq_count = projected.shape[1]
    bounds_list = [
        0,
        key_width,
        key_width + value_width,
        2 * key_width + value_width,
        3 * key_width + value_width,
        3 * key_width + 2 * value_width,
    ]

    def section_part(position, feature_lanes):
        picked = projected[:, :, bounds_list[position] : bounds_list[position + 1]].astype(
            jnp.float32
        )
        return picked.reshape(extent_rows, seq_count, heads_here, feature_lanes)

    queries = jax.nn.silu(section_part(0, KEY))
    values = section_part(1, VAL)
    shift = decay_shift.reshape(extent_rows, seq_count, heads_here, KEY)
    key_fwd = floor_gap[0].reshape(heads_here, KEY) * jax.nn.sigmoid(-section_part(2, KEY))
    key_bwd = floor_gap[1].reshape(heads_here, KEY) * jax.nn.sigmoid(-section_part(3, KEY))
    decay_fwd = jnp.log1p(-key_fwd) + shift
    decay_bwd = jnp.log1p(-key_bwd) + shift
    fwd_chain = prepare_chain(queries, key_fwd, values, decay_fwd)
    bwd_chain = prepare_chain(queries[::-1], key_bwd[::-1], values[::-1], decay_bwd[::-1])
    identity_pair = (jnp.zeros_like(fwd_chain[6]), jnp.zeros_like(fwd_chain[7]))
    fwd_in = carried_in((fwd_chain[6], fwd_chain[7]), "sp", combine, identity_pair, False)[1]
    bwd_in = carried_in((bwd_chain[6], bwd_chain[7]), "sp", combine, identity_pair, True)[1]
    out_fwd = local_pass(fwd_chain, fwd_in)
    out_bwd = local_pass(bwd_chain, bwd_in)
    combined = out_fwd + out_bwd[::-1]
    head_normed = (
        combined
        * lax.rsqrt(jnp.mean(combined * combined, axis=-1, keepdims=True) + norm_eps)
        * head_gain
    )
    gate_value = jax.nn.silu(projected[:, :, bounds_list[4] : bounds_list[5]].astype(jnp.float32))
    mixed = (head_normed.reshape(extent_rows, seq_count, value_width) * gate_value).astype(
        jnp.bfloat16
    )
    token_rows = lax.all_to_all(mixed, "tp", split_axis=0, concat_axis=2, tiled=True)
    flat_mixed = token_rows.reshape(-1, token_rows.shape[2])
    group_count = lax.axis_size("tp")
    w_columns = lax.all_gather(w_out, "sp", axis=1, tiled=True)
    w_full = lax.all_gather(w_columns, "tp", axis=0, tiled=True)
    accumulated_total = group_sums(flat_mixed, w_full, group_count)
    result = accumulated_total.reshape(token_rows.shape[0], token_rows.shape[1], -1)
    return result.astype(jnp.bfloat16)


MESH = pl.DeviceIdType.MESH
CORES = 2


def greet(peers):
    barrier = pltpu.get_barrier_semaphore()
    for peer in peers:
        pl.semaphore_signal(barrier, inc=1, device_id=peer, device_id_type=MESH)
    pl.semaphore_wait(barrier, len(peers))


def gather_phase(
    sizes,
    xn_ref,
    shift_ref,
    wq_ref,
    wv_ref,
    wf_ref,
    wb_ref,
    wg_ref,
    proj_ref,
    acts,
    weights,
    shifts,
    own_sem,
    az_sem,
    ax_sem,
    ac_sem,
    wz_sem,
    wy_sem,
    sz_sem,
):
    n_grp, n_sp, n_tp = sizes
    n_x = n_tp // CORES
    g = lax.axis_index("grp")
    s = lax.axis_index("sp")
    t = lax.axis_index("tp")
    x = t // CORES
    c = t % CORES
    seqs, span = xn_ref.shape[0], xn_ref.shape[1]
    depth = wq_ref.shape[0]
    part = depth // n_grp
    positions = shift_ref.shape[1]
    sources = (wq_ref, wv_ref, wf_ref, wb_ref, wg_ref)

    z_at = [s] + [lax.rem(s + k, n_sp) for k in range(1, n_sp)]
    z_from = [s] + [lax.rem(s + n_sp - k, n_sp) for k in range(1, n_sp)]
    x_at = [t] + [lax.rem(x + j, n_x) * CORES + c for j in range(1, n_x)]
    x_from = [t] + [lax.rem(x + n_x - j, n_x) * CORES + c for j in range(1, n_x)]
    twin = x * CORES + (1 - c)
    y_at = [g] + [lax.rem(g + m, n_grp) for m in range(1, n_grp)]
    y_from = [g] + [lax.rem(g + n_grp - m, n_grp) for m in range(1, n_grp)]

    def block(where_s, where_t):
        return acts.at[:, pl.ds(pl.multiple_of((where_s * n_tp + where_t) * span, span), span), :]

    def remote(src, dst, sems, index, peer):
        return pltpu.make_async_remote_copy(
            src_ref=src,
            dst_ref=dst,
            send_sem=sems.at[(0, *index)],
            recv_sem=sems.at[(1, *index)],
            device_id=peer,
            device_id_type=MESH,
        )

    def rows(where_s, where_g):
        return pl.ds(pl.multiple_of(where_s * depth + where_g * part, part), part)

    def lanes(where):
        return pl.ds(pl.multiple_of(where * KEY, KEY), KEY)

    mine = [
        pltpu.make_async_copy(
            w.at[:, lanes(s)],
            weights.at[pl.ds(pl.multiple_of(s * depth, depth), depth), pl.ds(p * KEY, KEY)],
            own_sem.at[p],
        )
        for p, w in enumerate(sources)
    ]
    mine.append(pltpu.make_async_copy(xn_ref, block(s, t), own_sem.at[len(sources)]))
    mine.append(
        pltpu.make_async_copy(
            shift_ref.at[:, :, lanes(s)],
            shifts.at[:, pl.ds(pl.multiple_of(s * positions, positions), positions), :],
            own_sem.at[len(sources) + 1],
        )
    )

    sent = []

    def go(copy):
        copy.start()
        sent.append(copy)
        return copy

    def slot(up, d):
        return 1 + d if up else n_sp + d

    def chain(up, d):
        step = -1 if up else 1
        there = s - step
        sends = jnp.logical_and(
            jnp.logical_and(there >= 0, there < n_sp),
            jnp.logical_and(s + step * d >= 0, s + step * d < n_sp),
        )
        gets = jnp.logical_and(s + step * (d + 1) >= 0, s + step * (d + 1) < n_sp)
        return there, s + step * d, sends, s + step * (d + 1), gets

    def act_move(up, d, from_own):
        there, origin, _, _, _ = chain(up, d)
        src = xn_ref if from_own else block(origin, t)
        return remote(src, block(origin, t), az_sem, (slot(up, d) - 1,), (g, there, t))

    def act_spread(kind, j, index, where_s, where_t, from_own):
        src = xn_ref if from_own else block(where_s, where_t)
        if kind == "x":
            return remote(src, block(where_s, where_t), ax_sem, (j - 1, index), (g, s, x_at[j]))
        return remote(src, block(where_s, where_t), ac_sem, (j, index), (g, s, twin))

    for up in (True, False):
        _, _, sends, _, _ = chain(up, 0)

        @pl.when(sends)
        def _():
            act_move(up, 0, True).start()

    for j in range(1, n_x):
        act_spread("x", j, 0, s, t, True).start()
    act_spread("c", 0, 0, s, t, True).start()
    for copy in mine:
        copy.start()

    w_z = {}

    def send_weights(p):
        for k in range(1, n_sp):
            w_z[k, p] = go(
                remote(
                    sources[p].at[pl.ds(pl.multiple_of(g * part, part), part), lanes(z_at[k])],
                    weights.at[rows(s, g), pl.ds(p * KEY, KEY)],
                    wz_sem,
                    (k - 1, p),
                    (g, z_at[k], t),
                )
            )

    w_y = {}

    def swap(p):
        for k in range(1, n_sp):
            w_z[k, p].wait_recv()
            here = weights.at[rows(z_from[k], g), pl.ds(p * KEY, KEY)]
            for m in range(1, n_grp):
                w_y[m, k, p] = go(remote(here, here, wy_sem, (m - 1, k - 1, p), (y_at[m], s, t)))

    queue = list(range(len(sources)))
    for d in range(n_sp - 1):
        if queue:
            send_weights(queue.pop(0))
        for up in (True, False):
            _, _, _, origin, gets = chain(up, d)

            @pl.when(gets)
            def _():
                act_move(up, d, False).wait_recv()
                if d + 1 < n_sp - 1:
                    _, _, sends, _, _ = chain(up, d + 1)

                    @pl.when(sends)
                    def _():
                        act_move(up, d + 1, False).start()

                for j in range(1, n_x):
                    act_spread("x", j, slot(up, d), origin, t, False).start()
                act_spread("c", 0, slot(up, d), origin, t, False).start()

        if d == n_sp - 2:
            for p in queue:
                send_weights(p)
            queue = []
        if d >= 1:
            swap(d - 1)

    s_z = {}
    for k in range(1, n_sp):
        s_z[k] = go(
            remote(
                shift_ref.at[:, :, lanes(z_at[k])],
                shifts.at[:, pl.ds(pl.multiple_of(s * positions, positions), positions), :],
                sz_sem,
                (k - 1,),
                (g, z_at[k], t),
            )
        )

    def each_block(visit, ds=None):
        if ds is None:
            visit(0, s)
        for d in range(n_sp - 1) if ds is None else ds:
            for up in (True, False):
                _, _, _, origin, gets = chain(up, d)

                @pl.when(gets)
                def _():
                    visit(slot(up, d), origin)

    def relay(index, origin):
        for j in range(1, n_x):
            act_spread("x", j, index, origin, t, False).wait_recv()
            act_spread("c", j, index, origin, x_from[j], False).start()

    relay(0, s)
    left = list(range(max(n_sp - 2, 0), len(sources)))
    for d in range(n_sp - 1):
        each_block(relay, [d])
        if left:
            swap(left.pop(0))
    for p in left:
        swap(p)
    for copy in mine:
        copy.wait()

    def joined(index, origin):
        for j in range(n_x):
            act_spread("c", j, index, origin, t, False).wait_recv()

    each_block(joined)
    for first in range(0, len(sources), 2):
        last = min(first + 2, len(sources))
        for (m, k, p), copy in w_y.items():
            if first <= p < last:
                copy.wait_recv()
        at = slice(first * KEY, last * KEY)

        def project(q, carry):
            proj_ref[q, :, at] = jnp.dot(
                acts[q], weights[:, at], preferred_element_type=jnp.float32
            ).astype(jnp.bfloat16)
            return carry

        lax.fori_loop(0, seqs, project, 0)
    for copy in s_z.values():
        copy.wait_recv()
    for d in range(n_sp - 1):
        for up in (True, False):
            _, _, sends, _, _ = chain(up, d)

            @pl.when(sends)
            def _():
                act_move(up, d, d == 0).wait_send()

    def gone(index, origin):
        for j in range(1, n_x):
            act_spread("x", j, index, origin, t, False).wait_send()
        for j in range(n_x):
            act_spread("c", j, index, origin, x_from[j], False).wait_send()

    each_block(gone)
    for copy in sent:
        copy.wait_send()


def recur_one(proj_ref, shift_ref, gap_ref, gain_ref, out_ref, i, own):
    f32 = jnp.float32
    bf16 = jnp.bfloat16
    length = proj_ref.shape[1]

    def cols(p):
        return proj_ref[i, :, p * KEY : (p + 1) * KEY]

    queries = cols(0).astype(f32)
    queries = queries * jax.nn.sigmoid(queries)
    values = cols(1)
    shift = shift_ref[i].astype(f32)
    row = lax.broadcasted_iota(jnp.int32, (length, length), 0)
    col = lax.broadcasted_iota(jnp.int32, (length, length), 1)
    near = row // BLOCK == col // BLOCK
    row = lax.broadcasted_iota(jnp.int32, (BLOCK, BLOCK), 0)
    col_b = lax.broadcasted_iota(jnp.int32, (BLOCK, BLOCK), 1)
    seen = [row >= col_b, row <= col_b]
    row_l = lax.broadcasted_iota(jnp.int32, (length, length), 0)
    order = [row_l >= col, row_l <= col]
    blocks = length // BLOCK
    keys, here = [], []
    for d in range(2):
        key = gap_ref[d : d + 1, own] * jax.nn.sigmoid(-cols(2 + d).astype(f32))
        decay = jnp.log1p(-key) + shift
        high = decay.astype(bf16)
        rest = decay - high.astype(f32)
        middle = rest.astype(bf16)
        low = (rest - middle.astype(f32)).astype(bf16)
        tri = jnp.where(jnp.logical_and(near, order[d]), 1.0, 0.0).astype(bf16)
        sums = jnp.dot(
            tri, jnp.concatenate([high, middle, low], axis=1), preferred_element_type=f32
        )
        here.append(sums[:, :KEY] + (sums[:, KEY : 2 * KEY] + sums[:, 2 * KEY :]))
        keys.append(key)
    state = [None, None]
    outs = [[None, None] for _ in range(blocks)]
    for step in range(blocks):
        for d in range(2):
            n = step if d == 0 else blocks - 1 - step
            at = slice(n * BLOCK, (n + 1) * BLOCK)
            q, k, v, h = queries[at], keys[d][at], values[at], here[d][at]
            edge = h[BLOCK - 1 : BLOCK] if d == 0 else h[0:1]
            anchor = h[BLOCK // 2 : BLOCK // 2 + 1]
            scores = lax.dot_general(
                (q * jnp.exp(h - anchor)).astype(bf16),
                (k * jnp.exp(anchor - h)).astype(bf16),
                (((1,), (1,)), ((), ())),
                preferred_element_type=f32,
            )
            scores = jnp.where(seen[d], scores, 0.0).astype(bf16)
            out = jnp.dot(scores, v, preferred_element_type=f32)
            if state[d] is not None:
                out = out + lax.dot_general(
                    (q * jnp.exp(h)).astype(bf16),
                    state[d].astype(bf16),
                    (((1,), (1,)), ((), ())),
                    preferred_element_type=f32,
                )
            outs[n][d] = out
            if step < blocks - 1:
                fresh = lax.dot_general(
                    v,
                    (k * jnp.exp(edge - h)).astype(bf16),
                    (((0,), (0,)), ((), ())),
                    preferred_element_type=f32,
                )
                state[d] = fresh if state[d] is None else state[d] * jnp.exp(edge) + fresh
    for n in range(blocks):
        out_ref[n * BLOCK : (n + 1) * BLOCK] = outs[n][0] + outs[n][1]
    combined = out_ref[...]
    normed = combined * lax.rsqrt(jnp.mean(combined * combined, axis=-1, keepdims=True) + norm_eps)
    gate = cols(4).astype(f32)
    return (normed * gain_ref[...] * (gate * jax.nn.sigmoid(gate))).astype(bf16)


def mix_phase(
    sizes,
    proj_ref,
    shift_ref,
    gap_ref,
    gain_ref,
    w_ref,
    out_ref,
    summed,
    heads,
    matrix,
    partial,
    landed,
    own_sem,
    w_sem,
    z_sem,
    c_sem,
    p_sem,
):
    n_grp, n_sp, n_tp = sizes
    n_x = n_tp // CORES
    g = lax.axis_index("grp")
    s = lax.axis_index("sp")
    t = lax.axis_index("tp")
    x = t // CORES
    c = t % CORES
    twin = x * CORES + (1 - c)
    seqs = proj_ref.shape[0]
    span = out_ref.shape[1]
    depth, width = w_ref.shape[0], w_ref.shape[1] // CORES
    half = seqs // 2
    z_at = [lax.rem(s + k, n_sp) for k in range(n_sp)]
    t_at = [lax.rem(t + j, n_tp) for j in range(n_tp)]
    others = [(k, j) for k in range(n_sp) for j in range(n_tp) if k or j]

    def lanes(where, size):
        return pl.ds(pl.multiple_of(where * size, size), size)

    def remote(src, dst, sems, index, peer):
        return pltpu.make_async_remote_copy(
            src_ref=src,
            dst_ref=dst,
            send_sem=sems.at[(0, *index)],
            recv_sem=sems.at[(1, *index)],
            device_id=peer,
            device_id_type=MESH,
        )

    w_rows = pl.ds(pl.multiple_of(c * depth, depth), depth)
    w_own = pltpu.make_async_copy(w_ref.at[:, lanes(c, width)], matrix.at[w_rows, :], own_sem)
    w_twin = remote(w_ref.at[:, lanes(1 - c, width)], matrix.at[w_rows, :], w_sem, (), (g, s, twin))
    w_own.start()
    w_twin.start()

    def head(q, where):
        return heads.at[q, :, lanes(c * n_sp + where, VAL)]

    def slot(up, d):
        return 1 + d if up else n_sp + d

    def inside(place):
        return jnp.logical_and(place >= 0, place < n_sp)

    def z_move(q, up, d):
        step = 1 if up else -1
        here = head(q, s - step * d)
        return remote(here, here, z_sem, (q, slot(up, d) - 1), (g, s + step, t))

    def z_sends(up, d):
        step = 1 if up else -1
        return jnp.logical_and(inside(s + step), inside(s - step * d))

    def z_gets(up, d):
        step = 1 if up else -1
        return inside(s - step * (d + 1))

    def c_move(q, index, origin):
        here = head(q, origin)
        return remote(here, here, c_sem, (q, index), (g, s, twin))

    def each(d, visit):
        for up in (True, False):

            @pl.when(z_gets(up, d))
            def _():
                visit(up, s - (d + 1) if up else s + (d + 1))

    def arrived(q, d):
        def visit(up, origin):
            z_move(q, up, d).wait_recv()
            if d + 1 < n_sp - 1:

                @pl.when(z_sends(up, d + 1))
                def _():
                    z_move(q, up, d + 1).start()

            c_move(q, slot(up, d), origin).start()

        each(d, visit)

    def advance(q, carry):
        heads[q, :, lanes(c * n_sp + s, VAL)] = recur_one(
            proj_ref, shift_ref, gap_ref, gain_ref, summed, q, lanes(s, KEY)
        )
        for up in (True, False):

            @pl.when(z_sends(up, 0))
            def _():
                z_move(q, up, 0).start()

        c_move(q, 0, s).start()
        for d in range(n_sp - 1):

            @pl.when(q >= d + 1)
            def _():
                arrived(q - (d + 1), d)

        return carry

    lax.fori_loop(0, seqs, advance, 0)

    def piece(where_s, where_t):
        return pl.ds(pl.multiple_of((where_s * n_tp + where_t) * span, span), span)

    def p_move(h, k, j):
        both = pl.ds(h * half, half)
        return remote(
            partial.at[both, piece(z_at[k], t_at[j]), :],
            landed.at[x, both, :, lanes(s * CORES + c, width)],
            p_sem,
            (h, k, j),
            (g, z_at[k], t_at[j]),
        )

    def finish(h):
        def one(q, carry):
            c_move(q, 0, s).wait_recv()
            for d in range(n_sp - 1):
                each(d, lambda up, origin: c_move(q, slot(up, d), origin).wait_recv())
            partial[q] = jnp.dot(
                heads[q], matrix[...], preferred_element_type=jnp.float32
            ).astype(jnp.bfloat16)
            return carry

        lax.fori_loop(h * half, (h + 1) * half, one, 0)
        for k, j in others:
            p_move(h, k, j).start()
        both = pl.ds(h * half, half)
        landed[x, both, :, lanes(s * CORES + c, width)] = partial[both, piece(s, t), :]

    w_own.wait()
    w_twin.wait_recv()
    pending = [
        (i - 1 - d, d)
        for i in range(seqs, seqs + n_sp - 1)
        for d in range(n_sp - 1)
        if 0 <= i - 1 - d < seqs
    ]
    early = [item for item in pending if item[0] < half]
    late = [item for item in pending if item[0] >= half]
    cut = pending.index(early[-1]) + 1 if early else 0
    for q, d in pending[:cut]:
        arrived(q, d)
    finish(0)
    for q, d in pending[cut:]:
        arrived(q, d)
    finish(1)
    for h in range(2):
        for k, j in others:
            p_move(h, k, j).wait_recv()
    total = landed[0].astype(jnp.float32)
    for j in range(1, n_x):
        total = total + landed[j].astype(jnp.float32)
    out_ref[...] = total.astype(jnp.bfloat16)

    w_twin.wait_send()

    def drain(q, carry):
        c_move(q, 0, s).wait_send()
        for d in range(n_sp - 1):
            each(d, lambda up, origin: c_move(q, slot(up, d), origin).wait_send())
            for up in (True, False):

                @pl.when(z_sends(up, d))
                def _():
                    z_move(q, up, d).wait_send()

        return carry

    lax.fori_loop(0, seqs, drain, 0)
    for h in range(2):
        for k, j in others:
            p_move(h, k, j).wait_send()


def layer_kernel(
    sizes,
    xn_ref,
    shift_ref,
    wq_ref,
    wv_ref,
    wf_ref,
    wb_ref,
    wg_ref,
    gap_ref,
    gain_ref,
    w_ref,
    out_ref,
    proj,
    acts,
    weights,
    shifts,
    summed,
    heads,
    matrix,
    partial,
    landed,
    own_sem,
    az_sem,
    ax_sem,
    ac_sem,
    wz_sem,
    wy_sem,
    sz_sem,
    mix_own_sem,
    mix_w_sem,
    mix_z_sem,
    mix_c_sem,
    mix_p_sem,
):
    n_grp, n_sp, n_tp = sizes
    g = lax.axis_index("grp")
    s = lax.axis_index("sp")
    t = lax.axis_index("tp")
    peers = [
        (g, lax.rem(s + k, n_sp), lax.rem(t + j, n_tp))
        for k in range(n_sp)
        for j in range(n_tp)
        if k or j
    ]
    peers += [(lax.rem(g + m, n_grp), s, t) for m in range(1, n_grp)]
    greet(peers)
    gather_phase(
        sizes,
        xn_ref,
        shift_ref,
        wq_ref,
        wv_ref,
        wf_ref,
        wb_ref,
        wg_ref,
        proj,
        acts,
        weights,
        shifts,
        own_sem,
        az_sem,
        ax_sem,
        ac_sem,
        wz_sem,
        wy_sem,
        sz_sem,
    )
    mix_phase(
        sizes,
        proj,
        shifts,
        gap_ref,
        gain_ref,
        w_ref,
        out_ref,
        summed,
        heads,
        matrix,
        partial,
        landed,
        mix_own_sem,
        mix_w_sem,
        mix_z_sem,
        mix_c_sem,
        mix_p_sem,
    )


def layer(sizes, xn, shift, sources, gap, gain, w_out):
    n_grp, n_sp, n_tp = sizes
    n_x = n_tp // CORES
    seqs, span, model = xn.shape
    length = n_sp * n_tp * span
    count = len(sources)
    depth, width = w_out.shape
    part = width // CORES
    dma = pltpu.SemaphoreType.DMA
    hbm = pl.BlockSpec(memory_space=pltpu.HBM)
    vmem = pl.BlockSpec(memory_space=pltpu.VMEM)
    return pl.pallas_call(
        functools.partial(layer_kernel, sizes),
        out_shape=jax.ShapeDtypeStruct((seqs, span, n_sp * width), jnp.bfloat16),
        in_specs=[hbm] * (2 + count) + [vmem, vmem, hbm],
        out_specs=vmem,
        scratch_shapes=[
            pltpu.VMEM((seqs, length, count * KEY), jnp.bfloat16),
            pltpu.VMEM((seqs, length, model), jnp.bfloat16),
            pltpu.VMEM((model, count * KEY), jnp.bfloat16),
            pltpu.VMEM((seqs, length, KEY), shift.dtype),
            pltpu.VMEM((length, VAL), jnp.float32),
            pltpu.VMEM((seqs, length, CORES * depth), jnp.bfloat16),
            pltpu.VMEM((CORES * depth, part), jnp.bfloat16),
            pltpu.VMEM((seqs, length, part), jnp.bfloat16),
            pltpu.VMEM((n_x, seqs, span, n_sp * width), jnp.bfloat16),
            dma((count + 2,)),
            dma((2, 2 * n_sp - 2)),
            dma((2, max(n_x - 1, 1), 2 * n_sp - 1)),
            dma((2, n_x, 2 * n_sp - 1)),
            dma((2, n_sp - 1, count)),
            dma((2, max(n_grp - 1, 1), n_sp - 1, count)),
            dma((2, n_sp - 1)),
            dma,
            dma((2,)),
            dma((2, seqs, 2 * n_sp - 2)),
            dma((2, seqs, 2 * n_sp - 1)),
            dma((2, 2, n_sp, n_tp)),
        ],
        compiler_params=pltpu.CompilerParams(
            collective_id=0, has_side_effects=True, vmem_limit_bytes=56 * 1024 * 1024
        ),
    )(xn, shift, *sources, gap, gain, w_out)


def head_shards(
    sizes,
    tokens,
    norm_gain,
    w_query,
    w_value,
    w_fwd_gate,
    w_bwd_gate,
    w_out_gate,
    floor_gap,
    decay_shift,
    head_gain,
    w_out,
):
    token_f32 = tokens.astype(jnp.float32)
    scale_rows = lax.rsqrt(jnp.mean(token_f32 * token_f32, axis=-1, keepdims=True) + norm_eps)
    normed = (token_f32 * scale_rows * norm_gain).astype(jnp.bfloat16)
    return layer(
        sizes,
        normed.transpose(1, 0, 2),
        decay_shift.astype(jnp.bfloat16).transpose(1, 0, 2),
        (w_query, w_value, w_fwd_gate, w_bwd_gate, w_out_gate),
        floor_gap,
        head_gain.reshape(1, VAL),
        w_out,
    ).transpose(1, 0, 2)


def by_heads(mesh):
    n_sp, n_tp = mesh.shape["sp"], mesh.shape["tp"]

    def run(*arrays):
        tokens, w_query = arrays[0], arrays[2]
        heads_here = w_query.shape[1] // KEY // n_tp
        span = tokens.shape[0] // (n_sp * n_tp)
        sizes = (mesh.shape["grp"], n_sp, n_tp)
        fits = heads_here == n_sp and n_sp > 1 and n_tp % CORES == 0 and span % 16 == 0
        fits = fits and tokens.shape[1] // sizes[0] % 2 == 0
        fits = fits and tokens.shape[0] % BLOCK == 0 and tokens.shape[0] <= 512
        body = functools.partial(head_shards, sizes) if fits else shards
        return mapped(body, mesh)(*arrays)

    return run


def mapped(body, mesh):
    return jax.shard_map(
        body,
        mesh=mesh,
        in_specs=(
            P(("sp", "tp"), "grp", None),
            P(),
            P("sp", "tp"),
            P("sp", "tp"),
            P("sp", "tp"),
            P("sp", "tp"),
            P("sp", "tp"),
            P(None, "tp"),
            P("sp", "grp", "tp"),
            P(),
            P("tp", "sp"),
        ),
        out_specs=P(("sp", "tp"), "grp", None),
        check_vma=False,
    )


def solution(mesh):
    return by_heads(mesh)
```

```python
import functools

import jax
import jax.numpy as jnp
from jax import lax
from jax.experimental import pallas as pl
from jax.experimental.pallas import tpu as pltpu
from jax.sharding import PartitionSpec as P

KEY = 128
VAL = 128
BLOCK = 64


norm_eps = 1e-06
highest = lax.Precision.HIGHEST


def carried_in(x, axis, join, neutral, backward):
    count = lax.axis_size(axis)
    place = lax.axis_index(axis)
    ahead = count - 1 - place if backward else place
    gathered = jax.tree.map(
        lambda a, kind: lax.all_gather(a.astype(kind), axis), x, (jnp.bfloat16, jnp.bfloat16)
    )
    state = jax.tree.map(lambda a, e: jnp.zeros_like(a) + jnp.asarray(e, a.dtype), x, neutral)

    def one(turn, state):
        source = count - 1 - turn if backward else turn
        return join(
            state,
            jax.tree.map(
                lambda a, own: lax.dynamic_index_in_dim(a, source, 0, False).astype(own.dtype),
                gathered,
                x,
            ),
        )

    return lax.fori_loop(0, ahead, one, state)


def split_blocks(array):
    return array.reshape(array.shape[0] // BLOCK, BLOCK, *array.shape[1:])


def prepare_chain(queries, key_cols, values, log_decay):
    query_blocks = split_blocks(queries)
    key_blocks = split_blocks(key_cols)
    value_blocks = split_blocks(values)
    running = jnp.cumsum(split_blocks(log_decay), axis=1)
    block_end = running[:, -1]
    block_state = jnp.einsum(
        "nsbhk,nsbhe->nbhke",
        key_blocks * jnp.exp(block_end[:, None] - running),
        value_blocks,
        precision=highest,
    )
    carry_state = jnp.zeros_like(block_state[0])
    log_total = jnp.zeros_like(block_end[0])
    offsets = [log_total]
    carry_state = jnp.exp(block_end[0])[..., None] * carry_state + block_state[0]
    log_total = block_end[0]
    return (
        query_blocks,
        key_blocks,
        value_blocks,
        running,
        block_state,
        jnp.stack(offsets),
        log_total,
        carry_state,
    )


def local_pass(chain, carry_state):
    query_blocks, key_blocks, value_blocks, running, block_state = (
        chain[0],
        chain[1],
        chain[2],
        chain[3],
        chain[4],
    )
    block_len = running.shape[1]
    earlier_mask = jnp.arange(block_len)[:, None] >= jnp.arange(block_len)[None, :]
    here = running[0]
    anchor = here[:1]
    query_scaled = query_blocks[0] * jnp.exp(here - anchor)
    key_scaled = key_blocks[0] * jnp.exp(anchor - here)
    scores = jnp.einsum("tbhk,sbhk->bhts", query_scaled, key_scaled, precision=highest)
    scores = jnp.where(earlier_mask, scores, 0.0)
    within = jnp.einsum("bhts,sbhe->tbhe", scores, value_blocks[0], precision=highest)
    carried = jnp.einsum(
        "tbhk,bhke->tbhe", query_blocks[0] * jnp.exp(here), carry_state, precision=highest
    )
    outputs = within + carried
    return outputs


def combine(earlier, later):
    return (earlier[0] + later[0], jnp.exp(later[0])[..., None] * earlier[1] + later[1])


def group_sums(flat_mixed, weight_lines, group_count):
    group_width = flat_mixed.shape[1] // group_count
    accumulated_total = jnp.zeros((flat_mixed.shape[0], weight_lines.shape[1]), jnp.float32)
    for tp_group in range(group_count):
        first_column = tp_group * group_width
        partial_value = jnp.dot(
            flat_mixed[:, first_column : first_column + group_width],
            weight_lines[first_column : first_column + group_width],
            preferred_element_type=jnp.float32,
        ).astype(jnp.bfloat16)
        accumulated_total = accumulated_total + lax.optimization_barrier(partial_value).astype(
            jnp.float32
        )
    return accumulated_total


def shards(
    tokens,
    norm_gain,
    w_query,
    w_value,
    w_fwd_gate,
    w_bwd_gate,
    w_out_gate,
    floor_gap,
    decay_shift,
    head_gain,
    w_out,
):
    token_f32 = tokens.astype(jnp.float32)
    scale_rows = lax.rsqrt(jnp.mean(token_f32 * token_f32, axis=-1, keepdims=True) + norm_eps)
    normed = (token_f32 * scale_rows * norm_gain).astype(jnp.bfloat16)
    weights = (
        lax.all_gather(w_query, "sp", axis=0, tiled=True),
        lax.all_gather(w_value, "sp", axis=0, tiled=True),
        lax.all_gather(w_fwd_gate, "sp", axis=0, tiled=True),
        lax.all_gather(w_bwd_gate, "sp", axis=0, tiled=True),
        lax.all_gather(w_out_gate, "sp", axis=0, tiled=True),
    )
    piece_rows = lax.all_gather(normed, "tp", axis=0, tiled=True)
    flat_rows = piece_rows.reshape(-1, piece_rows.shape[2])
    columns = [
        jnp.dot(flat_rows, matrix, preferred_element_type=jnp.float32).astype(jnp.bfloat16)
        for matrix in weights
    ]
    projected = lax.optimization_barrier(
        jnp.concatenate(columns, axis=1).reshape(piece_rows.shape[0], piece_rows.shape[1], -1)
    )
    key_width = w_query.shape[1]
    value_width = w_value.shape[1]
    heads_here = key_width // KEY
    extent_rows = projected.shape[0]
    seq_count = projected.shape[1]
    bounds_list = [
        0,
        key_width,
        key_width + value_width,
        2 * key_width + value_width,
        3 * key_width + value_width,
        3 * key_width + 2 * value_width,
    ]

    def section_part(position, feature_lanes):
        picked = projected[:, :, bounds_list[position] : bounds_list[position + 1]].astype(
            jnp.float32
        )
        return picked.reshape(extent_rows, seq_count, heads_here, feature_lanes)

    queries = jax.nn.silu(section_part(0, KEY))
    values = section_part(1, VAL)
    shift = decay_shift.reshape(extent_rows, seq_count, heads_here, KEY)
    key_fwd = floor_gap[0].reshape(heads_here, KEY) * jax.nn.sigmoid(-section_part(2, KEY))
    key_bwd = floor_gap[1].reshape(heads_here, KEY) * jax.nn.sigmoid(-section_part(3, KEY))
    decay_fwd = jnp.log1p(-key_fwd) + shift
    decay_bwd = jnp.log1p(-key_bwd) + shift
    fwd_chain = prepare_chain(queries, key_fwd, values, decay_fwd)
    bwd_chain = prepare_chain(queries[::-1], key_bwd[::-1], values[::-1], decay_bwd[::-1])
    identity_pair = (jnp.zeros_like(fwd_chain[6]), jnp.zeros_like(fwd_chain[7]))
    fwd_in = carried_in((fwd_chain[6], fwd_chain[7]), "sp", combine, identity_pair, False)[1]
    bwd_in = carried_in((bwd_chain[6], bwd_chain[7]), "sp", combine, identity_pair, True)[1]
    out_fwd = local_pass(fwd_chain, fwd_in)
    out_bwd = local_pass(bwd_chain, bwd_in)
    combined = out_fwd + out_bwd[::-1]
    head_normed = (
        combined
        * lax.rsqrt(jnp.mean(combined * combined, axis=-1, keepdims=True) + norm_eps)
        * head_gain
    )
    gate_value = jax.nn.silu(projected[:, :, bounds_list[4] : bounds_list[5]].astype(jnp.float32))
    mixed = (head_normed.reshape(extent_rows, seq_count, value_width) * gate_value).astype(
        jnp.bfloat16
    )
    token_rows = lax.all_to_all(mixed, "tp", split_axis=0, concat_axis=2, tiled=True)
    flat_mixed = token_rows.reshape(-1, token_rows.shape[2])
    group_count = lax.axis_size("tp")
    w_columns = lax.all_gather(w_out, "sp", axis=1, tiled=True)
    w_full = lax.all_gather(w_columns, "tp", axis=0, tiled=True)
    accumulated_total = group_sums(flat_mixed, w_full, group_count)
    result = accumulated_total.reshape(token_rows.shape[0], token_rows.shape[1], -1)
    return result.astype(jnp.bfloat16)


MESH = pl.DeviceIdType.MESH
CORES = 2


def greet(peers):
    barrier = pltpu.get_barrier_semaphore()
    for peer in peers:
        pl.semaphore_signal(barrier, inc=1, device_id=peer, device_id_type=MESH)
    pl.semaphore_wait(barrier, len(peers))


def gather_phase(
    sizes,
    xn_ref,
    shift_ref,
    wq_ref,
    wv_ref,
    wf_ref,
    wb_ref,
    wg_ref,
    proj_ref,
    acts,
    weights,
    shifts,
    own_sem,
    az_sem,
    ax_sem,
    ac_sem,
    wz_sem,
    wy_sem,
    sz_sem,
):
    n_grp, n_sp, n_tp = sizes
    n_x = n_tp // CORES
    g = lax.axis_index("grp")
    s = lax.axis_index("sp")
    t = lax.axis_index("tp")
    x = t // CORES
    c = t % CORES
    seqs, span = xn_ref.shape[0], xn_ref.shape[1]
    depth = wq_ref.shape[0]
    part = depth // n_grp
    positions = shift_ref.shape[1]
    sources = (wq_ref, wv_ref, wf_ref, wb_ref, wg_ref)

    z_at = [s] + [lax.rem(s + k, n_sp) for k in range(1, n_sp)]
    z_from = [s] + [lax.rem(s + n_sp - k, n_sp) for k in range(1, n_sp)]
    x_at = [t] + [lax.rem(x + j, n_x) * CORES + c for j in range(1, n_x)]
    x_from = [t] + [lax.rem(x + n_x - j, n_x) * CORES + c for j in range(1, n_x)]
    twin = x * CORES + (1 - c)
    y_at = [g] + [lax.rem(g + m, n_grp) for m in range(1, n_grp)]
    y_from = [g] + [lax.rem(g + n_grp - m, n_grp) for m in range(1, n_grp)]

    def block(where_s, where_t):
        return acts.at[:, pl.ds(pl.multiple_of((where_s * n_tp + where_t) * span, span), span), :]

    def remote(src, dst, sems, index, peer):
        return pltpu.make_async_remote_copy(
            src_ref=src,
            dst_ref=dst,
            send_sem=sems.at[(0, *index)],
            recv_sem=sems.at[(1, *index)],
            device_id=peer,
            device_id_type=MESH,
        )

    def rows(where_s, where_g):
        return pl.ds(pl.multiple_of(where_s * depth + where_g * part, part), part)

    def lanes(where):
        return pl.ds(pl.multiple_of(where * KEY, KEY), KEY)

    mine = [
        pltpu.make_async_copy(
            w.at[:, lanes(s)],
            weights.at[pl.ds(pl.multiple_of(s * depth, depth), depth), pl.ds(p * KEY, KEY)],
            own_sem.at[p],
        )
        for p, w in enumerate(sources)
    ]
    mine.append(
        pltpu.make_async_copy(
            shift_ref.at[:, :, lanes(s)],
            shifts.at[:, pl.ds(pl.multiple_of(s * positions, positions), positions), :],
            own_sem.at[len(sources)],
        )
    )

    sent = []

    def go(copy):
        copy.start()
        sent.append(copy)
        return copy

    def slot(up, d):
        return 1 + d if up else n_sp + d

    def chain(up, d):
        step = -1 if up else 1
        there = s - step
        sends = jnp.logical_and(
            jnp.logical_and(there >= 0, there < n_sp),
            jnp.logical_and(s + step * d >= 0, s + step * d < n_sp),
        )
        gets = jnp.logical_and(s + step * (d + 1) >= 0, s + step * (d + 1) < n_sp)
        return there, s + step * d, sends, s + step * (d + 1), gets

    def act_move(up, d, from_own):
        there, origin, _, _, _ = chain(up, d)
        src = block(origin, t)
        return remote(src, block(origin, t), az_sem, (slot(up, d) - 1,), (g, there, t))

    def act_spread(kind, j, index, where_s, where_t, from_own):
        src = block(where_s, where_t)
        if kind == "x":
            return remote(src, block(where_s, where_t), ax_sem, (j - 1, index), (g, s, x_at[j]))
        return remote(src, block(where_s, where_t), ac_sem, (j, index), (g, s, twin))

    for up in (True, False):
        _, _, sends, _, _ = chain(up, 0)

        @pl.when(sends)
        def _():
            act_move(up, 0, True).start()

    for j in range(1, n_x):
        act_spread("x", j, 0, s, t, True).start()
    act_spread("c", 0, 0, s, t, True).start()
    for copy in mine:
        copy.start()

    w_z = {}

    def send_weights(p):
        for k in range(1, n_sp):
            w_z[k, p] = go(
                remote(
                    sources[p].at[pl.ds(pl.multiple_of(g * part, part), part), lanes(z_at[k])],
                    weights.at[rows(s, g), pl.ds(p * KEY, KEY)],
                    wz_sem,
                    (k - 1, p),
                    (g, z_at[k], t),
                )
            )

    w_y = {}

    def swap(p):
        for k in range(1, n_sp):
            w_z[k, p].wait_recv()
            here = weights.at[rows(z_from[k], g), pl.ds(p * KEY, KEY)]
            for m in range(1, n_grp):
                w_y[m, k, p] = go(remote(here, here, wy_sem, (m - 1, k - 1, p), (y_at[m], s, t)))

    queue = list(range(len(sources)))
    for d in range(n_sp - 1):
        if queue and d >= 1:
            send_weights(queue.pop(0))
        for up in (True, False):
            _, _, _, origin, gets = chain(up, d)

            @pl.when(gets)
            def _():
                act_move(up, d, False).wait_recv()
                if d + 1 < n_sp - 1:
                    _, _, sends, _, _ = chain(up, d + 1)

                    @pl.when(sends)
                    def _():
                        act_move(up, d + 1, False).start()

                for j in range(1, n_x):
                    act_spread("x", j, slot(up, d), origin, t, False).start()
                act_spread("c", 0, slot(up, d), origin, t, False).start()

        if d == n_sp - 2:
            for p in queue:
                send_weights(p)
            queue = []
        if d >= 2:
            swap(d - 2)

    s_z = {}
    for k in range(1, n_sp):
        s_z[k] = go(
            remote(
                shift_ref.at[:, :, lanes(z_at[k])],
                shifts.at[:, pl.ds(pl.multiple_of(s * positions, positions), positions), :],
                sz_sem,
                (k - 1,),
                (g, z_at[k], t),
            )
        )

    def each_block(visit, ds=None):
        if ds is None:
            visit(0, s)
        for d in range(n_sp - 1) if ds is None else ds:
            for up in (True, False):
                _, _, _, origin, gets = chain(up, d)

                @pl.when(gets)
                def _():
                    visit(slot(up, d), origin)

    def relay(index, origin):
        for j in range(1, n_x):
            act_spread("x", j, index, origin, t, False).wait_recv()
            act_spread("c", j, index, origin, x_from[j], False).start()

    relay(0, s)
    left = list(range(max(n_sp - 3, 0), len(sources)))
    for d in range(n_sp - 1):
        each_block(relay, [d])
        if left:
            swap(left.pop(0))
    for p in left:
        swap(p)
    for copy in mine:
        copy.wait()

    def joined(index, origin):
        for j in range(n_x):
            act_spread("c", j, index, origin, t, False).wait_recv()

    each_block(joined)
    for first in range(0, len(sources), 2):
        last = min(first + 2, len(sources))
        for (m, k, p), copy in w_y.items():
            if first <= p < last:
                copy.wait_recv()
        at = slice(first * KEY, last * KEY)

        def project(q, carry):
            proj_ref[q, :, at] = jnp.dot(
                acts[q], weights[:, at], preferred_element_type=jnp.float32
            ).astype(jnp.bfloat16)
            return carry

        lax.fori_loop(0, seqs, project, 0)
    for copy in s_z.values():
        copy.wait_recv()
    for d in range(n_sp - 1):
        for up in (True, False):
            _, _, sends, _, _ = chain(up, d)

            @pl.when(sends)
            def _():
                act_move(up, d, d == 0).wait_send()

    def gone(index, origin):
        for j in range(1, n_x):
            act_spread("x", j, index, origin, t, False).wait_send()
        for j in range(n_x):
            act_spread("c", j, index, origin, x_from[j], False).wait_send()

    each_block(gone)
    for copy in sent:
        copy.wait_send()


def recur_one(proj_ref, shift_ref, gap_ref, gain_ref, out_ref, i, own):
    f32 = jnp.float32
    bf16 = jnp.bfloat16
    length = proj_ref.shape[1]

    def cols(p):
        return proj_ref[i, :, p * KEY : (p + 1) * KEY]

    queries = cols(0).astype(f32)
    queries = queries * jax.nn.sigmoid(queries)
    values = cols(1)
    shift = shift_ref[i].astype(f32)
    row = lax.broadcasted_iota(jnp.int32, (length, length), 0)
    col = lax.broadcasted_iota(jnp.int32, (length, length), 1)
    near = row // BLOCK == col // BLOCK
    row = lax.broadcasted_iota(jnp.int32, (BLOCK, BLOCK), 0)
    col_b = lax.broadcasted_iota(jnp.int32, (BLOCK, BLOCK), 1)
    seen = [row >= col_b, row <= col_b]
    row_l = lax.broadcasted_iota(jnp.int32, (length, length), 0)
    order = [row_l >= col, row_l <= col]
    blocks = length // BLOCK
    keys, here = [], []
    for d in range(2):
        key = gap_ref[d : d + 1, own] * jax.nn.sigmoid(-cols(2 + d).astype(f32))
        decay = jnp.log1p(-key) + shift
        high = decay.astype(bf16)
        rest = decay - high.astype(f32)
        middle = rest.astype(bf16)
        low = (rest - middle.astype(f32)).astype(bf16)
        tri = jnp.where(jnp.logical_and(near, order[d]), 1.0, 0.0).astype(bf16)
        sums = jnp.dot(
            tri, jnp.concatenate([high, middle, low], axis=1), preferred_element_type=f32
        )
        here.append(sums[:, :KEY] + (sums[:, KEY : 2 * KEY] + sums[:, 2 * KEY :]))
        keys.append(key)
    state = [None, None]
    outs = [[None, None] for _ in range(blocks)]
    for step in range(blocks):
        for d in range(2):
            n = step if d == 0 else blocks - 1 - step
            at = slice(n * BLOCK, (n + 1) * BLOCK)
            q, k, v, h = queries[at], keys[d][at], values[at], here[d][at]
            edge = h[BLOCK - 1 : BLOCK] if d == 0 else h[0:1]
            anchor = h[BLOCK // 2 : BLOCK // 2 + 1]
            scores = lax.dot_general(
                (q * jnp.exp(h - anchor)).astype(bf16),
                (k * jnp.exp(anchor - h)).astype(bf16),
                (((1,), (1,)), ((), ())),
                preferred_element_type=f32,
            )
            scores = jnp.where(seen[d], scores, 0.0).astype(bf16)
            out = jnp.dot(scores, v, preferred_element_type=f32)
            if state[d] is not None:
                out = out + lax.dot_general(
                    (q * jnp.exp(h)).astype(bf16),
                    state[d].astype(bf16),
                    (((1,), (1,)), ((), ())),
                    preferred_element_type=f32,
                )
            outs[n][d] = out
            if step < blocks - 1:
                fresh = lax.dot_general(
                    v,
                    (k * jnp.exp(edge - h)).astype(bf16),
                    (((0,), (0,)), ((), ())),
                    preferred_element_type=f32,
                )
                state[d] = fresh if state[d] is None else state[d] * jnp.exp(edge) + fresh
    for n in range(blocks):
        out_ref[n * BLOCK : (n + 1) * BLOCK] = outs[n][0] + outs[n][1]
    combined = out_ref[...]
    normed = combined * lax.rsqrt(jnp.mean(combined * combined, axis=-1, keepdims=True) + norm_eps)
    gate = cols(4).astype(f32)
    return (normed * gain_ref[...] * (gate * jax.nn.sigmoid(gate))).astype(bf16)


def mix_phase(
    sizes,
    proj_ref,
    shift_ref,
    gap_ref,
    gain_ref,
    w_ref,
    out_ref,
    summed,
    heads,
    matrix,
    partial,
    landed,
    own_sem,
    w_sem,
    z_sem,
    c_sem,
    p_sem,
):
    n_grp, n_sp, n_tp = sizes
    n_x = n_tp // CORES
    g = lax.axis_index("grp")
    s = lax.axis_index("sp")
    t = lax.axis_index("tp")
    x = t // CORES
    c = t % CORES
    twin = x * CORES + (1 - c)
    seqs = proj_ref.shape[0]
    span = out_ref.shape[1]
    depth, width = w_ref.shape[0], w_ref.shape[1] // CORES
    half = seqs // 2
    z_at = [lax.rem(s + k, n_sp) for k in range(n_sp)]
    t_at = [lax.rem(t + j, n_tp) for j in range(n_tp)]
    others = [(k, j) for k in range(n_sp) for j in range(n_tp) if k or j]

    def lanes(where, size):
        return pl.ds(pl.multiple_of(where * size, size), size)

    def remote(src, dst, sems, index, peer):
        return pltpu.make_async_remote_copy(
            src_ref=src,
            dst_ref=dst,
            send_sem=sems.at[(0, *index)],
            recv_sem=sems.at[(1, *index)],
            device_id=peer,
            device_id_type=MESH,
        )

    w_rows = pl.ds(pl.multiple_of(c * depth, depth), depth)
    w_own = pltpu.make_async_copy(w_ref.at[:, lanes(c, width)], matrix.at[w_rows, :], own_sem)
    w_twin = remote(w_ref.at[:, lanes(1 - c, width)], matrix.at[w_rows, :], w_sem, (), (g, s, twin))
    w_own.start()
    w_twin.start()

    def head(q, where):
        return heads.at[q, :, lanes(c * n_sp + where, VAL)]

    def slot(up, d):
        return 1 + d if up else n_sp + d

    def inside(place):
        return jnp.logical_and(place >= 0, place < n_sp)

    def z_move(q, up, d):
        step = 1 if up else -1
        here = head(q, s - step * d)
        return remote(here, here, z_sem, (q, slot(up, d) - 1), (g, s + step, t))

    def z_sends(up, d):
        step = 1 if up else -1
        return jnp.logical_and(inside(s + step), inside(s - step * d))

    def z_gets(up, d):
        step = 1 if up else -1
        return inside(s - step * (d + 1))

    def c_move(q, index, origin):
        here = head(q, origin)
        return remote(here, here, c_sem, (q, index), (g, s, twin))

    def each(d, visit):
        for up in (True, False):

            @pl.when(z_gets(up, d))
            def _():
                visit(up, s - (d + 1) if up else s + (d + 1))

    def arrived(q, d):
        def visit(up, origin):
            z_move(q, up, d).wait_recv()
            if d + 1 < n_sp - 1:

                @pl.when(z_sends(up, d + 1))
                def _():
                    z_move(q, up, d + 1).start()

            c_move(q, slot(up, d), origin).start()

        each(d, visit)

    def advance(q, carry):
        heads[q, :, lanes(c * n_sp + s, VAL)] = recur_one(
            proj_ref, shift_ref, gap_ref, gain_ref, summed, q, lanes(s, KEY)
        )
        for up in (True, False):

            @pl.when(z_sends(up, 0))
            def _():
                z_move(q, up, 0).start()

        c_move(q, 0, s).start()
        for d in range(n_sp - 1):

            @pl.when(q >= d + 1)
            def _():
                arrived(q - (d + 1), d)

        return carry

    lax.fori_loop(0, seqs, advance, 0)

    def piece(where_s, where_t):
        return pl.ds(pl.multiple_of((where_s * n_tp + where_t) * span, span), span)

    def p_move(h, k, j):
        both = pl.ds(h * half, half)
        return remote(
            partial.at[both, piece(z_at[k], t_at[j]), :],
            landed.at[x, both, :, lanes(s * CORES + c, width)],
            p_sem,
            (h, k, j),
            (g, z_at[k], t_at[j]),
        )

    def finish(h):
        def one(q, carry):
            c_move(q, 0, s).wait_recv()
            for d in range(n_sp - 1):
                each(d, lambda up, origin: c_move(q, slot(up, d), origin).wait_recv())
            partial[q] = jnp.dot(
                heads[q], matrix[...], preferred_element_type=jnp.float32
            ).astype(jnp.bfloat16)
            return carry

        lax.fori_loop(h * half, (h + 1) * half, one, 0)
        for k, j in others:
            p_move(h, k, j).start()
        both = pl.ds(h * half, half)
        landed[x, both, :, lanes(s * CORES + c, width)] = partial[both, piece(s, t), :]

    w_own.wait()
    w_twin.wait_recv()
    pending = [
        (i - 1 - d, d)
        for i in range(seqs, seqs + n_sp - 1)
        for d in range(n_sp - 1)
        if 0 <= i - 1 - d < seqs
    ]
    early = [item for item in pending if item[0] < half]
    late = [item for item in pending if item[0] >= half]
    cut = pending.index(early[-1]) + 1 if early else 0
    for q, d in pending[:cut]:
        arrived(q, d)
    finish(0)
    for q, d in pending[cut:]:
        arrived(q, d)
    finish(1)
    for h in range(2):
        for k, j in others:
            p_move(h, k, j).wait_recv()
    total = landed[0].astype(jnp.float32)
    for j in range(1, n_x):
        total = total + landed[j].astype(jnp.float32)
    out_ref[...] = total.astype(jnp.bfloat16)

    w_twin.wait_send()

    def drain(q, carry):
        c_move(q, 0, s).wait_send()
        for d in range(n_sp - 1):
            each(d, lambda up, origin: c_move(q, slot(up, d), origin).wait_send())
            for up in (True, False):

                @pl.when(z_sends(up, d))
                def _():
                    z_move(q, up, d).wait_send()

        return carry

    lax.fori_loop(0, seqs, drain, 0)
    for h in range(2):
        for k, j in others:
            p_move(h, k, j).wait_send()


def layer_kernel(
    sizes,
    xn_ref,
    norm_ref,
    shift_ref,
    wq_ref,
    wv_ref,
    wf_ref,
    wb_ref,
    wg_ref,
    gap_ref,
    gain_ref,
    w_ref,
    out_ref,
    proj,
    acts,
    weights,
    shifts,
    summed,
    heads,
    matrix,
    partial,
    landed,
    own_sem,
    az_sem,
    ax_sem,
    ac_sem,
    wz_sem,
    wy_sem,
    sz_sem,
    mix_own_sem,
    mix_w_sem,
    mix_z_sem,
    mix_c_sem,
    mix_p_sem,
):
    n_grp, n_sp, n_tp = sizes
    g = lax.axis_index("grp")
    s = lax.axis_index("sp")
    t = lax.axis_index("tp")
    peers = [
        (g, lax.rem(s + k, n_sp), lax.rem(t + j, n_tp))
        for k in range(n_sp)
        for j in range(n_tp)
        if k or j
    ]
    peers += [(lax.rem(g + m, n_grp), s, t) for m in range(1, n_grp)]
    span = xn_ref.shape[1]
    rows = xn_ref[...].astype(jnp.float32)
    scale = lax.rsqrt(jnp.mean(rows * rows, axis=-1, keepdims=True) + norm_eps)
    acts[:, pl.ds(pl.multiple_of((s * n_tp + t) * span, span), span), :] = (
        rows * scale * norm_ref[...]
    ).astype(jnp.bfloat16)
    greet(peers)
    gather_phase(
        sizes,
        xn_ref,
        shift_ref,
        wq_ref,
        wv_ref,
        wf_ref,
        wb_ref,
        wg_ref,
        proj,
        acts,
        weights,
        shifts,
        own_sem,
        az_sem,
        ax_sem,
        ac_sem,
        wz_sem,
        wy_sem,
        sz_sem,
    )
    mix_phase(
        sizes,
        proj,
        shifts,
        gap_ref,
        gain_ref,
        w_ref,
        out_ref,
        summed,
        heads,
        matrix,
        partial,
        landed,
        mix_own_sem,
        mix_w_sem,
        mix_z_sem,
        mix_c_sem,
        mix_p_sem,
    )


def layer(sizes, xn, norm_gain, shift, sources, gap, gain, w_out):
    n_grp, n_sp, n_tp = sizes
    n_x = n_tp // CORES
    seqs, span, model = xn.shape
    length = n_sp * n_tp * span
    count = len(sources)
    depth, width = w_out.shape
    part = width // CORES
    dma = pltpu.SemaphoreType.DMA
    hbm = pl.BlockSpec(memory_space=pltpu.HBM)
    vmem = pl.BlockSpec(memory_space=pltpu.VMEM)
    return pl.pallas_call(
        functools.partial(layer_kernel, sizes),
        out_shape=jax.ShapeDtypeStruct((seqs, span, n_sp * width), jnp.bfloat16),
        in_specs=[vmem, vmem] + [hbm] * (1 + count) + [vmem, vmem, hbm],
        out_specs=vmem,
        scratch_shapes=[
            pltpu.VMEM((seqs, length, count * KEY), jnp.bfloat16),
            pltpu.VMEM((seqs, length, model), jnp.bfloat16),
            pltpu.VMEM((model, count * KEY), jnp.bfloat16),
            pltpu.VMEM((seqs, length, KEY), shift.dtype),
            pltpu.VMEM((length, VAL), jnp.float32),
            pltpu.VMEM((seqs, length, CORES * depth), jnp.bfloat16),
            pltpu.VMEM((CORES * depth, part), jnp.bfloat16),
            pltpu.VMEM((seqs, length, part), jnp.bfloat16),
            pltpu.VMEM((n_x, seqs, span, n_sp * width), jnp.bfloat16),
            dma((count + 1,)),
            dma((2, 2 * n_sp - 2)),
            dma((2, max(n_x - 1, 1), 2 * n_sp - 1)),
            dma((2, n_x, 2 * n_sp - 1)),
            dma((2, n_sp - 1, count)),
            dma((2, max(n_grp - 1, 1), n_sp - 1, count)),
            dma((2, n_sp - 1)),
            dma,
            dma((2,)),
            dma((2, seqs, 2 * n_sp - 2)),
            dma((2, seqs, 2 * n_sp - 1)),
            dma((2, 2, n_sp, n_tp)),
        ],
        compiler_params=pltpu.CompilerParams(
            collective_id=0, has_side_effects=True, vmem_limit_bytes=56 * 1024 * 1024
        ),
    )(xn, norm_gain, shift, *sources, gap, gain, w_out)


def head_shards(
    sizes,
    tokens,
    norm_gain,
    w_query,
    w_value,
    w_fwd_gate,
    w_bwd_gate,
    w_out_gate,
    floor_gap,
    decay_shift,
    head_gain,
    w_out,
):
    return layer(
        sizes,
        tokens.transpose(1, 0, 2),
        norm_gain.reshape(1, 1, -1),
        decay_shift.astype(jnp.bfloat16).transpose(1, 0, 2),
        (w_query, w_value, w_fwd_gate, w_bwd_gate, w_out_gate),
        floor_gap,
        head_gain.reshape(1, VAL),
        w_out,
    ).transpose(1, 0, 2)


def by_heads(mesh):
    n_sp, n_tp = mesh.shape["sp"], mesh.shape["tp"]

    def run(*arrays):
        tokens, w_query = arrays[0], arrays[2]
        heads_here = w_query.shape[1] // KEY // n_tp
        span = tokens.shape[0] // (n_sp * n_tp)
        sizes = (mesh.shape["grp"], n_sp, n_tp)
        fits = heads_here == n_sp and n_sp > 1 and n_tp % CORES == 0 and span % 16 == 0
        fits = fits and tokens.shape[1] // sizes[0] % 2 == 0
        fits = fits and tokens.shape[0] % BLOCK == 0 and tokens.shape[0] <= 512
        body = functools.partial(head_shards, sizes) if fits else shards
        return mapped(body, mesh)(*arrays)

    return run


def mapped(body, mesh):
    return jax.shard_map(
        body,
        mesh=mesh,
        in_specs=(
            P(("sp", "tp"), "grp", None),
            P(),
            P("sp", "tp"),
            P("sp", "tp"),
            P("sp", "tp"),
            P("sp", "tp"),
            P("sp", "tp"),
            P(None, "tp"),
            P("sp", "grp", "tp"),
            P(),
            P("tp", "sp"),
        ),
        out_specs=P(("sp", "tp"), "grp", None),
        check_vma=False,
    )


def solution(mesh):
    return by_heads(mesh)
```
